512 devices in a mesh: sp: 64 (over z, y), fs: 4 (over x), tp: 2 (over core).
Axes of the slice: x: 4, y: 8, z: 8, core: 2. Of those that a mesh axis runs over, the one named last changes fastest.
Arguments:
- tokens: bfloat16 [16384, 2048], P('sp', ('fs', 'tp')), may hold values from -500 to 500
- norm_gain: float32 [2048], replicated, may hold values from 0.1 to 1.9
- query_w: bfloat16 [2048, 1024], P('sp', ('fs', 'tp')), may hold values from -1 to 1
- key_w: bfloat16 [2048, 512], P('sp', ('fs', 'tp')), may hold values from -1 to 1
- value_w: bfloat16 [2048, 512], P('sp', ('fs', 'tp')), may hold values from -0.125 to 0.125
- recept_w: bfloat16 [2048, 1024], P('sp', ('fs', 'tp')), may hold values from -0.125 to 0.125
- rec_key_w: bfloat16 [2048, 1024], P('sp', ('fs', 'tp')), may hold values from -0.125 to 0.125
- rec_value_w: bfloat16 [2048, 1024], P('sp', ('fs', 'tp')), may hold values from -0.125 to 0.125
- decay_down: bfloat16 [2048, 64], replicated, may hold values from -0.125 to 0.125
- decay_up: bfloat16 [64, 1024], replicated, may hold values from -1 to 1
- decay_base: float32 [16, 16384], P(('fs', 'tp'), 'sp'), may hold values from -14 to 0
- learn_rate: float32 [1024], P(('fs', 'tp')), may hold values from 0.1 to 1
- query_gain: float32 [64], replicated, may hold values from 0 to 7
- key_gain: float32 [64], replicated, may hold values from 0 to 7
- sink_logit: float32 [16], P(('fs', 'tp')), may hold values from 1 to 5
- group_gain: float32 [1024], P(('fs', 'tp')), may hold values from 0.1 to 1.9
- out_att_w: bfloat16 [1024, 2048], P(('fs', 'tp'), 'sp'), may hold values from -0.75 to 0.75
- out_rec_w: bfloat16 [1024, 2048], P(('fs', 'tp'), 'sp'), may hold values from -0.1875 to 0.1875
Outputs:
- mixed: bfloat16 [16384, 2048], P(('sp', 'fs', 'tp'))
- row_lse: float32 [16, 16384], P(('fs', 'tp'), 'sp')
The draws below stay inside these ranges and needn't reach their ends.
All inputs are finite; a program needn't handle non-finite values.
Results may differ from the reference program's by a relative error of at most 0.015.
Values may be sent and summed in bfloat16 or wider, within the bound.
No kernel may reach another device: no remote copies, remote signals or barrier semaphores. Data moves between devices by JAX's collectives and lax.ppermute only.
A program may use at most 64 MiB of HBM per device.

```python
import math
import jax
import jax.numpy as jnp
from jax import lax

D = 2048
HEAD = 64
ATT_HEADS = 16
KV_HEADS = 8
RECURRENT_HEADS = 16
DECAY_RANK = 64
WINDOW = 128
TOK = 256
SEQUENCE_LENGTH = 16384
ATT_WIDTH = 1024
KV_WIDTH = 512
REC_WIDTH = 1024
N_FS = 4
N_TP = 2


def draw_tokens(key, part):
    normal_key = jax.random.fold_in(key, 101)
    base_values = jnp.clip(jax.random.normal(normal_key, (SEQUENCE_LENGTH, D), jnp.float32), -5.0, 5.0)
    column_scale = jnp.exp(jnp.log(10.0) * jnp.arange(D, dtype=jnp.float32) / D)
    row_scale = jnp.exp(jax.random.uniform(jax.random.fold_in(key, 102), (SEQUENCE_LENGTH, 1), jnp.float32, 0.0, 2.3))
    return (base_values * column_scale[None, :] * row_scale).astype(jnp.bfloat16)


def draw_head_gain(key, salt):
    gain_key = jax.random.fold_in(key, salt)
    gain_vec = 1.0 + 0.18 * jnp.clip(jax.random.normal(gain_key, (HEAD,), jnp.float32), -4.5, 4.5)
    return gain_vec


def draw_query_gain(key, part):
    return draw_head_gain(key, 103)


def draw_key_gain(key, part):
    return draw_head_gain(key, 104)


def draw_attention_pair(key):
    scale_val = 1.0 / jnp.sqrt(jnp.float32(D))
    query_part = jnp.clip(jax.random.normal(jax.random.fold_in(key, 201), (D, ATT_WIDTH), jnp.float32), -5.0, 5.0) * scale_val
    key_part = jnp.clip(jax.random.normal(jax.random.fold_in(key, 202), (D, KV_WIDTH), jnp.float32), -5.0, 5.0) * scale_val
    return (query_part, key_part)


def draw_query_w(key, part):
    return draw_attention_pair(key)[0].astype(jnp.bfloat16)


def draw_key_w(key, part):
    return draw_attention_pair(key)[1].astype(jnp.bfloat16)


def draw_decay_base(key, part):
    fast_share = 0.5
    fast_heads = jax.random.uniform(jax.random.fold_in(key, 301), (RECURRENT_HEADS, 1), jnp.float32) < fast_share
    head_rate = jnp.where(fast_heads, 1.0 / 40.0, 0.4 / SEQUENCE_LENGTH)
    block_factor = jnp.exp(jax.random.uniform(jax.random.fold_in(key, 302), (RECURRENT_HEADS, SEQUENCE_LENGTH // TOK), jnp.float32, -0.7, 0.7))
    steady_frequency = head_rate * jnp.repeat(block_factor, TOK, axis=1)
    spike_locations = jax.random.randint(jax.random.fold_in(key, 303), (3,), 0, SEQUENCE_LENGTH)
    spike_frequency = jnp.exp(jax.random.uniform(jax.random.fold_in(key, 304), (RECURRENT_HEADS, 3), jnp.float32, -1.9, -0.7))
    token_places = jnp.arange(SEQUENCE_LENGTH)
    spike_events = token_places[None, None, :] == spike_locations[None, :, None]
    spike_pattern = jnp.sum(jnp.where(spike_events, spike_frequency[:, :, None], 0.0), axis=1)
    combined_frequency = jnp.where(spike_pattern > 0.0, spike_pattern, steady_frequency)
    return jnp.log(combined_frequency)


def block_levels(stream_key, dims, shards, low, high):
    factor_of = 1.0
    for axis_at, shards_of in shards:
        steps = jax.random.uniform(jax.random.fold_in(jax.random.fold_in(stream_key, 6), axis_at), (shards_of,), jnp.float32, low / len(shards), high / len(shards))
        factor_of = factor_of * jnp.repeat(jnp.exp(steps), dims[axis_at] // shards_of).reshape((-1,) + (1,) * (len(dims) - 1 - axis_at))
    return factor_of


def gaussian(rng, shape, deviation, limit, split=(), kind=jnp.bfloat16):
    result = jax.random.normal(rng, shape, jnp.float32) * deviation
    if len(split) > 0:
        result = block_levels(rng, shape, split, -0.22, 0.18) * result
    return jnp.clip(result, min=-limit, max=limit).astype(kind)


def setup_inputs(seed: int = 0) -> dict:
    seeds = jax.random.split(jax.random.key(seed), 19)
    return {
        "tokens": draw_tokens(jax.random.fold_in(seeds[18], 71), 0),
        "norm_gain": jnp.clip(1.0 + 0.18 * jax.random.normal(seeds[1], (D,), jnp.float32), 0.1, 1.9),
        "query_w": draw_query_w(jax.random.fold_in(seeds[18], 71), 0),
        "key_w": draw_key_w(jax.random.fold_in(seeds[18], 71), 0),
        "value_w": gaussian(seeds[4], (D, KV_WIDTH), D ** -0.5, 0.125, ((0, 64), (1, 8))),
        "recept_w": gaussian(seeds[5], (D, REC_WIDTH), D ** -0.5, 0.125, ((0, 64), (1, 8))),
        "rec_key_w": gaussian(seeds[6], (D, REC_WIDTH), D ** -0.5, 0.125, ((0, 64), (1, 8))),
        "rec_value_w": gaussian(seeds[7], (D, REC_WIDTH), D ** -0.5, 0.125, ((0, 64), (1, 8))),
        "decay_down": gaussian(seeds[8], (D, DECAY_RANK), D ** -0.5, 0.125),
        "decay_up": gaussian(seeds[9], (DECAY_RANK, REC_WIDTH), (DECAY_RANK // 2) ** -0.5, 1.0),
        "decay_base": draw_decay_base(jax.random.fold_in(seeds[18], 71), 0),
        "learn_rate": jnp.clip(0.1 + 0.9 * jax.random.uniform(seeds[11], (REC_WIDTH,), jnp.float32) ** block_levels(seeds[11], (REC_WIDTH,), ((0, 8),), -0.2, 0.2), 0.1, 1.0),
        "query_gain": draw_query_gain(jax.random.fold_in(seeds[18], 71), 0),
        "key_gain": draw_key_gain(jax.random.fold_in(seeds[18], 71), 0),
        "sink_logit": jnp.clip(1.0 + 4.0 * jax.random.uniform(seeds[14], (ATT_HEADS,), jnp.float32) ** block_levels(seeds[14], (ATT_HEADS,), ((0, 8),), -0.2, 0.2), 1.0, 5.0),
        "group_gain": jnp.clip(1.0 + 0.18 * jax.random.normal(seeds[15], (REC_WIDTH,), jnp.float32), 0.1, 1.9),
        "out_att_w": gaussian(seeds[16], (ATT_WIDTH, D), (ATT_WIDTH // 16) ** -0.5, 0.75, ((0, 8), (1, 64))),
        "out_rec_w": gaussian(seeds[17], (REC_WIDTH, D), REC_WIDTH ** -0.5, 0.1875, ((0, 8), (1, 64))),
    }


NORM_EPS = 1e-06
KEY_EPS = 1e-06
GROUP_EPS = 0.00064
EXACT_PRECISION = lax.Precision.HIGHEST

def project(hidden, weight_mat):
    product = jnp.dot(hidden, weight_mat, preferred_element_type=jnp.float32)
    return lax.optimization_barrier(product.astype(jnp.bfloat16))

def head_rms(values, gain_vec, num_heads):
    shaped = values.astype(jnp.float32).reshape(values.shape[0], num_heads, HEAD)
    mean_sq = lax.optimization_barrier(jnp.mean(shaped * shaped, axis=-1, keepdims=True))
    normed = (shaped * lax.rsqrt(mean_sq + NORM_EPS) * gain_vec).astype(jnp.bfloat16)
    return lax.optimization_barrier(normed)

def window_head(query_head, key_head, value_head, sink_value):
    blocks = query_head.shape[0] // WINDOW
    query_blocks = query_head.astype(jnp.float32).reshape(blocks, WINDOW, HEAD)
    key_blocks = key_head.astype(jnp.float32).reshape(blocks, WINDOW, HEAD)
    value_blocks = value_head.astype(jnp.float32).reshape(blocks, WINDOW, HEAD)
    zero_block = jnp.zeros((1, WINDOW, HEAD), jnp.float32)
    key_band = jnp.concatenate([jnp.concatenate([zero_block, key_blocks[:-1]], axis=0), key_blocks], axis=1)
    value_band = jnp.concatenate([jnp.concatenate([zero_block, value_blocks[:-1]], axis=0), value_blocks], axis=1)
    scores = jnp.einsum('nqd,nsd->nqs', query_blocks, key_band) * (1.0 / math.sqrt(HEAD))
    lag_table = jnp.arange(WINDOW)[:, None] + WINDOW - jnp.arange(2 * WINDOW)[None, :]
    key_place = (jnp.arange(blocks)[:, None] - 1) * WINDOW + jnp.arange(2 * WINDOW)[None, :]
    allowed = ((lag_table >= 0) & (lag_table < WINDOW))[None, :, :] & (key_place >= 0)[:, None, :]
    masked = jnp.where(allowed, scores, -jnp.inf)
    row_top = jnp.maximum(lax.optimization_barrier(jnp.max(masked, axis=-1, keepdims=True)), sink_value)
    weight = jnp.where(allowed, jnp.exp(masked - row_top), 0.0)
    row_total = lax.optimization_barrier(jnp.sum(weight, axis=-1, keepdims=True)) + jnp.exp(sink_value - row_top)
    head_lse = (row_top + jnp.log(row_total)).reshape(-1)
    att_probs = lax.optimization_barrier((weight / row_total).astype(jnp.bfloat16)).astype(jnp.float32)
    head_out = jnp.einsum('nqs,nsd->nqd', att_probs, value_band).reshape(-1, HEAD)
    return (head_out.astype(jnp.bfloat16), head_lse)

def attention(query_n, key_n, att_values, sink_logit):
    group_size = ATT_HEADS // KV_HEADS
    query_heads = query_n.transpose(1, 0, 2)
    key_heads = jnp.repeat(key_n.transpose(1, 0, 2), group_size, axis=0)
    value_heads = jnp.repeat(att_values.reshape(SEQUENCE_LENGTH, KV_HEADS, HEAD).transpose(1, 0, 2), group_size, axis=0)
    head_outs, head_lse = lax.map(lambda packed: window_head(*packed), (query_heads, key_heads, value_heads, sink_logit))
    return (head_outs.transpose(1, 0, 2).reshape(SEQUENCE_LENGTH, ATT_WIDTH), head_lse)

def recurrence(reads, rec_keys, rec_values, log_decay, learn_rate, group_gain):
    read_vals = reads.astype(jnp.float32).reshape(SEQUENCE_LENGTH, RECURRENT_HEADS, HEAD)
    key_vals = rec_keys.astype(jnp.float32).reshape(SEQUENCE_LENGTH, RECURRENT_HEADS, HEAD)
    value_vals = rec_values.astype(jnp.float32).reshape(SEQUENCE_LENGTH, RECURRENT_HEADS, HEAD)
    unit_key = key_vals * lax.rsqrt(lax.optimization_barrier(jnp.sum(key_vals * key_vals, axis=-1, keepdims=True)) + KEY_EPS)
    removal = -unit_key
    writing = unit_key * learn_rate.reshape(RECURRENT_HEADS, HEAD)
    decay_vals = jnp.exp(log_decay.reshape(SEQUENCE_LENGTH, RECURRENT_HEADS, HEAD))

    def token_step(head_state, inputs):
        read_now, decay_now, key_now, current_value, removal_now, writing_now = inputs
        along_vec = jnp.einsum('hij,hj->hi', head_state, removal_now, precision=EXACT_PRECISION)
        head_state = head_state * decay_now[:, None, :] + along_vec[:, :, None] * writing_now[:, None, :] + current_value[:, :, None] * key_now[:, None, :]
        return (head_state, jnp.einsum('hij,hj->hi', head_state, read_now, precision=EXACT_PRECISION))
    zero_state = jnp.zeros((RECURRENT_HEADS, HEAD, HEAD), jnp.float32)
    _, read_out = lax.scan(token_step, zero_state, (read_vals, decay_vals, key_vals, value_vals, removal, writing))
    mean_val = lax.optimization_barrier(jnp.mean(read_out, axis=-1, keepdims=True))
    centered = read_out - mean_val
    variance = lax.optimization_barrier(jnp.mean(centered * centered, axis=-1, keepdims=True))
    normed = (centered * lax.rsqrt(variance + GROUP_EPS)).reshape(SEQUENCE_LENGTH, REC_WIDTH) * group_gain
    return normed.astype(jnp.bfloat16)

def reference(tokens, norm_gain, query_w, key_w, value_w, recept_w, rec_key_w, rec_value_w, decay_down, decay_up, decay_base, learn_rate, query_gain, key_gain, sink_logit, group_gain, out_att_w, out_rec_w):
    full_rows = tokens.astype(jnp.float32)
    mean_sq = lax.optimization_barrier(jnp.mean(full_rows * full_rows, axis=-1, keepdims=True))
    hidden = (full_rows * lax.rsqrt(mean_sq + NORM_EPS) * norm_gain).astype(jnp.bfloat16)
    query_rows = project(hidden, query_w)
    key_rows = project(hidden, key_w)
    att_values = project(hidden, value_w)
    reads = project(hidden, recept_w)
    rec_keys = project(hidden, rec_key_w)
    rec_values = project(hidden, rec_value_w)
    decay_low = jnp.tanh(jnp.dot(hidden, decay_down, preferred_element_type=jnp.float32)).astype(jnp.bfloat16)
    decay_rate = jnp.dot(decay_low, decay_up, preferred_element_type=jnp.float32) + jnp.repeat(decay_base.T, HEAD, axis=1)
    log_decay = -jnp.exp(decay_rate)
    query_n = head_rms(query_rows, query_gain, ATT_HEADS)
    key_n = head_rms(key_rows, key_gain, KV_HEADS)
    att_mix, row_lse = attention(query_n, key_n, att_values, sink_logit)
    rec_mix = recurrence(reads, rec_keys, rec_values, log_decay, learn_rate, group_gain)
    groups = N_FS * N_TP
    att_span = ATT_WIDTH // groups
    rec_span = REC_WIDTH // groups
    acc_total = jnp.zeros((SEQUENCE_LENGTH, D), jnp.float32)
    for group_index in range(groups):
        att_lo = group_index * att_span
        rec_lo = group_index * rec_span
        group_partial = jnp.dot(att_mix[:, att_lo:att_lo + att_span], out_att_w[att_lo:att_lo + att_span], preferred_element_type=jnp.float32) + jnp.dot(rec_mix[:, rec_lo:rec_lo + rec_span], out_rec_w[rec_lo:rec_lo + rec_span], preferred_element_type=jnp.float32)
        acc_total = acc_total + lax.optimization_barrier(group_partial.astype(jnp.bfloat16)).astype(jnp.float32)
    return (acc_total.astype(jnp.bfloat16), row_lse)
```

```python
import functools
import math

import jax
import jax.numpy as jnp
from jax import lax
from jax.experimental import pallas as pl
from jax.experimental.pallas import tpu as pltpu
from jax.sharding import Mesh
from jax.sharding import PartitionSpec as P

HEAD = 64
WINDOW = 128
CHUNK = 32
SP = ("sp_0", "sp_1")
SP_FS_TP = ("sp_0", "sp_1", "fs", "tp")
F32 = jnp.float32
BF16 = jnp.bfloat16

NORM_EPS = 1e-06
KEY_EPS = 1e-06
GROUP_EPS = 0.00064
DECAY_FLOOR = -104.0

NT = (((1,), (1,)), ((), ()))
TN = (((0,), (0,)), ((), ()))


def ring_shift(array, axis, by):
    devices = lax.axis_size(axis)
    return lax.ppermute(array, axis, [(i, (i + by) % devices) for i in range(devices)])


def passed_along(array, axis, by):
    devices = lax.axis_size(axis)
    pairs = [(i, i + by) for i in range(devices) if 0 <= i + by < devices]
    return lax.ppermute(array, axis, pairs)


def from_everyone(array, axis):
    copies = jnp.broadcast_to(array, (lax.axis_size(axis), *array.shape))
    return lax.all_to_all(copies, axis, split_axis=0, concat_axis=0, tiled=True)


def call(kernel, outs, scratch=(), flops=0, smem=0, name=None):
    def run(*args):
        specs = [
            pl.BlockSpec(memory_space=pltpu.SMEM if i < smem else pltpu.VMEM)
            for i in range(len(args))
        ]
        return pl.pallas_call(
            kernel,
            out_shape=[jax.ShapeDtypeStruct(s, d) for s, d in outs],
            in_specs=specs,
            out_specs=[pl.BlockSpec(memory_space=pltpu.VMEM)] * len(outs),
            scratch_shapes=list(scratch),
            cost_estimate=pl.CostEstimate(flops=flops, bytes_accessed=1 << 21, transcendentals=0),
            compiler_params=pltpu.CompilerParams(vmem_limit_bytes=40 << 20),
            name=name,
        )(*args)

    return run


def dot(a, b, dims=(((1,), (0,)), ((), ()))):
    return lax.dot_general(a.astype(BF16), b.astype(BF16), dims, preferred_element_type=F32)


def hidden_kernel(place, own, next_, before, across, other, gain, down, up, base, hid, ld, cum, rest):
    x = place[0]
    core = place[1]
    rows = own.shape[0]
    blocks = [own, before, across, next_]
    sums = jnp.zeros((rows, 1), F32)
    for k in range(4):
        mine = blocks[k][...].astype(F32)
        theirs = other[k].astype(F32)
        sums += jnp.sum(mine * mine + theirs * theirs, axis=1, keepdims=True)
    width = own.shape[1]
    scale = lax.rsqrt(sums / (8 * width) + NORM_EPS)
    low = jnp.zeros((rows, down.shape[1]), F32)
    for k in range(4):
        chip = lax.rem(x + k, 4)
        for c, block in ((core, blocks[k][...]), (1 - core, other[k])):
            at = pl.multiple_of((chip * 2 + c) * width, width)
            h = (block.astype(F32) * scale * gain[:, pl.ds(at, width)]).astype(BF16)
            hid[:, pl.ds(at, width)] = h
            low += jnp.dot(h, down[pl.ds(at, width), :], preferred_element_type=F32)
    low = jnp.tanh(low).astype(BF16)
    rate = lax.dot_general(up[...], low, (((0,), (1,)), ((), ())), preferred_element_type=F32)
    heads = base.shape[0]
    base_rows = jnp.concatenate(
        [jnp.broadcast_to(base[h : h + 1, :], (HEAD, rows)) for h in range(heads)], axis=0
    )
    log_decay = jnp.maximum(-jnp.exp(rate + base_rows), DECAY_FLOOR)
    ld[...] = log_decay
    lane = lax.broadcasted_iota(jnp.int32, log_decay.shape, 1) % CHUNK
    total, after = log_decay, log_decay
    step = 1
    while step < CHUNK:
        total = total + jnp.where(lane >= step, pltpu.roll(total, step, 1), 0.0)
        after = after + jnp.where(lane < CHUNK - step, pltpu.roll(after, rows - step, 1), 0.0)
        step *= 2
    cum[...] = total
    rest[...] = after - log_decay


def head_rows(h):
    return slice(h * HEAD, (h + 1) * HEAD)


def band_tables(left, right, start, end, rate, first, heads):
    rows = left.shape[1]
    dist = (
        lax.broadcasted_iota(jnp.int32, (CHUNK, rows), 1) % CHUNK
        - lax.broadcasted_iota(jnp.int32, (CHUNK, rows), 0)
    )
    plain, rated = [], []
    for h in range(heads):
        sl = head_rows(h)
        l, r, s, e = left[sl, :], right[sl, :], start[sl, :], end[sl, :]
        speed = jnp.broadcast_to(rate[sl, :], l.shape)
        t_plain = jnp.zeros((CHUNK, rows), F32)
        t_rated = jnp.zeros((CHUNK, rows), F32)
        for d in range(first, CHUNK):
            rd = r if d == 0 else pltpu.roll(r, d, 1)
            ed = e if d == 0 else pltpu.roll(e, d, 1)
            x = l * rd * jnp.exp(s - ed)
            here = dist == d
            t_plain = jnp.where(here, jnp.sum(x, axis=0, keepdims=True), t_plain)
            t_rated = jnp.where(here, jnp.sum(x * speed, axis=0, keepdims=True), t_rated)
        plain.append(t_plain)
        rated.append(t_rated)
    return plain, rated


def in_chunks(table):
    rows = table.shape[1]
    tall = jnp.concatenate([table] * (rows // CHUNK), axis=0)
    same = (
        lax.broadcasted_iota(jnp.int32, (rows, rows), 0) // CHUNK
        == lax.broadcasted_iota(jnp.int32, (rows, rows), 1) // CHUNK
    )
    return jnp.where(same, tall, 0.0).astype(BF16)


def by_chunk(array):
    rows = array.shape[1]
    chunk = lax.broadcasted_iota(jnp.int32, array.shape, 1) // CHUNK
    return jnp.concatenate(
        [jnp.where(chunk == c, array, 0.0).astype(BF16) for c in range(rows // CHUNK)], axis=0
    )


def state_kernel(hid, w, lr, ld, cum, rest, ends, unit, value, solved, starts, dec):
    rows = hid.shape[0]
    heads = lr.shape[0] // HEAD
    span = heads * HEAD
    kv = jnp.dot(hid[...], w[...], preferred_element_type=F32).astype(BF16).astype(F32)
    kv_t = kv.T
    for h in range(heads):
        k = kv_t[head_rows(h), :]
        square = jnp.sum(k * k, axis=0, keepdims=True) + KEY_EPS
        inv = lax.rsqrt(square)
        unit[head_rows(h), :] = k * inv
        value[head_rows(h), :] = kv_t[span + h * HEAD : span + (h + 1) * HEAD, :] * (square * inv)
    cum_all = cum[...]
    prev = cum_all - ld[...]
    dec[...] = jnp.exp(cum_all).T
    u = unit[...]
    v = value[...]
    plain, rated = band_tables(u, u, prev, cum_all, lr, 1, heads)
    reach = jnp.exp(prev)
    x, q = [], []
    for h in range(heads):
        sl = head_rows(h)
        x.append(jnp.concatenate([-u[sl, :] * reach[sl, :], -dot(v[sl, :], in_chunks(plain[h]))], axis=0))
        q.append(in_chunks(-rated[h]))
    power = 1
    while power < CHUNK:
        for h in range(heads):
            x[h] = x[h] + dot(x[h], q[h])
        power *= 2
        if power < CHUNK:
            for h in range(heads):
                q[h] = dot(q[h], q[h]).astype(BF16)
    left = jnp.exp(rest[...])
    chunks = rows // CHUNK
    grow = []
    for h in range(heads):
        sl = head_rows(h)
        solved[h] = x[h].astype(BF16)
        out_u = u[sl, :] * left[sl, :]
        out_b = out_u * lr[sl, :]
        g = dot(x[h], by_chunk(out_b), NT)
        g_low = g[HEAD:, :] + dot(v[sl, :], by_chunk(out_u), NT)
        grow.append((g[:HEAD, :].astype(BF16), g_low))
    eye = (
        lax.broadcasted_iota(jnp.int32, (2 * HEAD, HEAD), 0)
        == lax.broadcasted_iota(jnp.int32, (2 * HEAD, HEAD), 1)
    ).astype(F32)
    state = [eye] * heads
    zero = jnp.zeros((HEAD, HEAD), F32)
    for c in range(chunks):
        at = slice(c * HEAD, (c + 1) * HEAD)
        last = c * CHUNK + CHUNK - 1
        for h in range(heads):
            low = state[h].astype(BF16)
            starts[h, :, at] = low
            kept = state[h] * dec[last : last + 1, head_rows(h)]
            added = jnp.concatenate([zero, grow[h][1][:, at]], axis=0)
            state[h] = kept + added + jnp.dot(low, grow[h][0][:, at], preferred_element_type=F32)
    for h in range(heads):
        ends[h] = state[h].astype(BF16)


def read_kernel(hid, w, lr, cum, unit, value, solved, starts, out):
    rows = hid.shape[0]
    heads = lr.shape[0] // HEAD
    reads = jnp.dot(hid[...], w[...], preferred_element_type=F32).astype(BF16).astype(F32)
    r = reads.T
    cum_all = cum[...]
    plain, rated = band_tables(r, unit[...], cum_all, cum_all, lr, 0, heads)
    reach = r * jnp.exp(cum_all)
    for h in range(heads):
        sl = head_rows(h)
        mixed = dot(solved[h], in_chunks(rated[h]))
        query = mixed[:HEAD, :] + reach[sl, :]
        local = mixed[HEAD:, :] + dot(value[sl, :], in_chunks(plain[h]))
        both = dot(starts[h], by_chunk(query))
        out[h, :HEAD, :] = both[:HEAD, :]
        out[h, HEAD:, :] = both[HEAD:, :] + local


def chain(earlier, later):
    moved = jnp.dot(earlier.astype(BF16), later[:HEAD, :], preferred_element_type=F32)
    return moved + jnp.concatenate([jnp.zeros((HEAD, HEAD), F32), later[HEAD:, :].astype(F32)], axis=0)


def row_kernel(place, pieces, total_out, inside_out):
    devices, heads = pieces.shape[0], pieces.shape[1]
    eye = (
        lax.broadcasted_iota(jnp.int32, (2 * HEAD, HEAD), 0)
        == lax.broadcasted_iota(jnp.int32, (2 * HEAD, HEAD), 1)
    ).astype(F32)
    total = [eye] * heads
    inside = [eye] * heads
    for k in range(devices):
        passed = k < place[0]
        for h in range(heads):
            later = pieces[k, h]
            total[h] = later.astype(F32) if k == 0 else chain(total[h], later)
            inside[h] = jnp.where(passed, total[h], inside[h])
    for h in range(heads):
        total_out[h] = total[h].astype(BF16)
        inside_out[h] = inside[h].astype(BF16)


def final_kernel(place, pieces, inside, local, gain, att, w, out):
    devices, heads = pieces.shape[0], pieces.shape[1]
    state = [jnp.zeros((HEAD, HEAD), F32)] * heads
    for k in range(devices - 1):
        passed = k < place[0]
        for h in range(heads):
            new = jnp.dot(state[h].astype(BF16), pieces[k, h, :HEAD, :], preferred_element_type=F32)
            new = new + pieces[k, h, HEAD:, :].astype(F32)
            state[h] = jnp.where(passed, new, state[h])
    rows = []
    for h in range(heads):
        start = jnp.dot(state[h].astype(BF16), inside[h, :HEAD, :], preferred_element_type=F32)
        start = start + inside[h, HEAD:, :].astype(F32)
        y = dot(start, local[h, :HEAD, :]) + local[h, HEAD:, :]
        centered = y - jnp.mean(y, axis=0, keepdims=True)
        variance = jnp.mean(centered * centered, axis=0, keepdims=True)
        rows.append(centered * lax.rsqrt(variance + GROUP_EPS) * gain[head_rows(h), :])
    rec = jnp.concatenate(rows, axis=0).T.astype(BF16)
    mix = jnp.concatenate([att[...], rec], axis=1)
    groups, width = out.shape[0], 512
    size = out.shape[1]
    for n in range(w.shape[0] // width):
        at = slice(n * width, (n + 1) * width)
        part = lax.dot_general(mix, w[at, :], NT, preferred_element_type=F32).astype(BF16)
        for g in range(groups):
            out[g, :, at] = part[g * size : (g + 1) * size, :]


def head_rms(values, gain_vec, num_heads):
    shaped = values.astype(jnp.float32).reshape(values.shape[0], num_heads, HEAD)
    mean_sq = jnp.mean(shaped * shaped, axis=-1, keepdims=True)
    return (shaped * lax.rsqrt(mean_sq + NORM_EPS) * gain_vec).astype(jnp.bfloat16)


def attend(query_rows, key_rows, value_rows, query_gain, key_gain, sink_logit):
    num_rows = query_rows.shape[0]
    num_heads = query_rows.shape[1] // HEAD
    kv_heads = key_rows.shape[1] // HEAD
    group_size = num_heads // kv_heads
    blocks = num_rows // WINDOW
    query_n = head_rms(query_rows, query_gain, num_heads).reshape(
        blocks, WINDOW, kv_heads, group_size, HEAD
    )
    key_n = head_rms(key_rows, key_gain, kv_heads).reshape(num_rows, kv_heads * HEAD)
    paired = jnp.concatenate([key_n, value_rows], axis=1)
    before = passed_along(paired[num_rows - WINDOW :], SP, 1)
    current = paired.reshape(blocks, WINDOW, 2 * kv_heads * HEAD)
    previous = jnp.concatenate([before[None], current[:-1]], axis=0)
    key_band = jnp.concatenate([previous, current], axis=1).reshape(
        blocks, 2 * WINDOW, 2, kv_heads, HEAD
    )
    scores = jnp.einsum(
        "nqkgd,nskd->nkgqs", query_n, key_band[:, :, 0], preferred_element_type=jnp.float32
    ) * (1.0 / math.sqrt(HEAD))
    offset = lax.axis_index(SP) * num_rows
    lag_table = (
        lax.broadcasted_iota(jnp.int32, (WINDOW, 2 * WINDOW), 0)
        + WINDOW
        - lax.broadcasted_iota(jnp.int32, (WINDOW, 2 * WINDOW), 1)
    )
    key_place = (
        offset
        + (lax.broadcasted_iota(jnp.int32, (blocks, 2 * WINDOW), 0) - 1) * WINDOW
        + lax.broadcasted_iota(jnp.int32, (blocks, 2 * WINDOW), 1)
    )
    allowed = ((lag_table >= 0) & (lag_table < WINDOW))[None, :, :] & (key_place >= 0)[:, None, :]
    allowed = allowed[:, None, None]
    sink_cols = sink_logit.reshape(kv_heads, group_size)[None, :, :, None, None]
    masked = jnp.where(allowed, scores, -jnp.inf)
    row_top = jnp.maximum(jnp.max(masked, axis=-1, keepdims=True), sink_cols)
    weight = jnp.where(allowed, jnp.exp(masked - row_top), 0.0)
    row_total = jnp.sum(weight, axis=-1, keepdims=True) + jnp.exp(sink_cols - row_top)
    row_lse = (
        (row_top + jnp.log(row_total))[..., 0].transpose(1, 2, 0, 3).reshape(num_heads, num_rows)
    )
    att_probs = (weight / row_total).astype(jnp.bfloat16)
    mixed_heads = jnp.einsum(
        "nkgqs,nskd->nqkgd", att_probs, key_band[:, :, 1], preferred_element_type=jnp.float32
    )
    return (mixed_heads.reshape(num_rows, num_heads * HEAD).astype(jnp.bfloat16), row_lse)


def per_device(
    tokens,
    norm_gain,
    query_w,
    key_w,
    value_w,
    recept_w,
    rec_key_w,
    rec_value_w,
    decay_down,
    decay_up,
    decay_base,
    learn_rate,
    query_gain,
    key_gain,
    sink_logit,
    group_gain,
    out_att_w,
    out_rec_w,
):
    rows = tokens.shape[0]
    span = recept_w.shape[1]
    heads = span // HEAD
    features = norm_gain.shape[0]
    groups = lax.axis_size(("fs", "tp"))
    place_zy = [lax.axis_index(a).astype(jnp.int32).reshape(1) for a in SP]

    own = jnp.concatenate(
        [rec_key_w, rec_value_w, recept_w, query_w, key_w, value_w, out_att_w.T, out_rec_w.T], axis=1
    )
    column = from_everyone(own, "sp_1").reshape(-1, own.shape[1])
    state_w = from_everyone(column[:, : 2 * span], "sp_0").reshape(features, 2 * span)
    other_w = lax.all_gather(column[:, 2 * span :], "sp_0", axis=0, tiled=True)

    before = ring_shift(tokens, "fs", -1)
    across = ring_shift(tokens, "fs", 2)
    next_ = ring_shift(tokens, "fs", 1)
    other = ring_shift(jnp.stack([tokens, before, across, next_]), "tp", 1)

    place_xc = jnp.stack([lax.axis_index("fs"), lax.axis_index("tp")]).astype(jnp.int32)
    decay_cols = lax.dynamic_slice_in_dim(
        decay_up, lax.axis_index(("fs", "tp")) * span, span, 1
    )
    flat = (span, rows)
    hid, ld, cum, rest = call(
        hidden_kernel,
        [((rows, features), BF16), (flat, F32), (flat, F32), (flat, F32)],
        smem=1,
        flops=1 << 27,
        name="hidden",
    )(
        place_xc, tokens, next_, before, across, other, norm_gain.reshape(1, -1), decay_down, decay_cols, decay_base
    )

    lr = learn_rate.reshape(span, 1)
    chunks = rows // CHUNK
    ends, unit, value, solved, starts = call(
        state_kernel,
        [
            ((heads, 2 * HEAD, HEAD), BF16),
            (flat, F32),
            (flat, F32),
            ((heads, 2 * HEAD, rows), BF16),
            ((heads, 2 * HEAD, chunks * HEAD), BF16),
        ],
        scratch=[pltpu.VMEM((rows, span), F32)],
        flops=1 << 31,
        name="state",
    )(hid, state_w, lr, ld, cum, rest)

    row_pieces = from_everyone(ends, "sp_1")
    row_total, inside = call(
        row_kernel,
        [((heads, 2 * HEAD, HEAD), BF16)] * 2,
        smem=1,
        flops=1 << 27,
        name="rowchain",
    )(place_zy[1], row_pieces)
    all_pieces = from_everyone(row_total, "sp_0")

    (local,) = call(
        read_kernel, [((heads, 2 * HEAD, rows), F32)], flops=1 << 31, name="reads"
    )(hid, other_w[:, :span], lr, cum, unit, value, solved, starts)
    q_w, kv_w = query_w.shape[1], key_w.shape[1]
    att_w = other_w[:, span : span + q_w + 2 * kv_w]
    att_in = lax.optimization_barrier(
        jnp.dot(hid, att_w, preferred_element_type=F32).astype(BF16)
    )
    att_mix, row_lse = attend(
        att_in[:, :q_w], att_in[:, q_w : q_w + kv_w], att_in[:, q_w + kv_w :], query_gain, key_gain, sink_logit
    )
    out_w = other_w[:, span + q_w + 2 * kv_w :]

    (partial,) = call(
        final_kernel,
        [((groups, rows // groups, features), BF16)],
        smem=1,
        flops=1 << 30,
        name="final",
    )(place_zy[0], all_pieces, inside, local, group_gain.reshape(span, 1), att_mix, out_w)
    tiles = lax.all_to_all(partial, ("fs", "tp"), 0, 0, tiled=True)
    mixed = jnp.sum(tiles.astype(F32), axis=0).astype(BF16)
    return (mixed, row_lse)


def solution(mesh):
    split = Mesh(
        mesh.devices.reshape(8, 8, mesh.shape["fs"], mesh.shape["tp"]), ("sp_0", "sp_1", "fs", "tp")
    )
    in_specs = (
        P(SP, ("fs", "tp")),
        P(),
        P(SP, ("fs", "tp")),
        P(SP, ("fs", "tp")),
        P(SP, ("fs", "tp")),
        P(SP, ("fs", "tp")),
        P(SP, ("fs", "tp")),
        P(SP, ("fs", "tp")),
        P(),
        P(),
        P(("fs", "tp"), SP),
        P(("fs", "tp")),
        P(),
        P(),
        P(("fs", "tp")),
        P(("fs", "tp")),
        P(("fs", "tp"), SP),
        P(("fs", "tp"), SP),
    )
    out_specs = (P(SP_FS_TP, None), P(("fs", "tp"), SP))
    return jax.shard_map(
        per_device, mesh=split, in_specs=in_specs, out_specs=out_specs, check_vma=False
    )
```

```python
import math

import jax
import jax.numpy as jnp
from jax import lax
from jax.experimental import pallas as pl
from jax.experimental.pallas import tpu as pltpu
from jax.sharding import Mesh
from jax.sharding import PartitionSpec as P

HEAD = 64
WINDOW = 128
CHUNK = 32
SP = ("sp_0", "sp_1")
SP_FS_TP = ("sp_0", "sp_1", "fs", "tp")
F32 = jnp.float32
BF16 = jnp.bfloat16

NORM_EPS = 1e-06
KEY_EPS = 1e-06
GROUP_EPS = 0.00064
DECAY_FLOOR = -104.0

NT = (((1,), (1,)), ((), ()))
TN = (((0,), (0,)), ((), ()))


def ring_shift(array, axis, by):
    devices = lax.axis_size(axis)
    return lax.ppermute(array, axis, [(i, (i + by) % devices) for i in range(devices)])


def passed_along(array, axis, by):
    devices = lax.axis_size(axis)
    pairs = [(i, i + by) for i in range(devices) if 0 <= i + by < devices]
    return lax.ppermute(array, axis, pairs)


def from_everyone(array, axis):
    copies = jnp.broadcast_to(array, (lax.axis_size(axis), *array.shape))
    return lax.all_to_all(copies, axis, split_axis=0, concat_axis=0, tiled=True)


class Fetched:
    def __init__(self, source, target, sem):
        self.copy = pltpu.make_async_copy(source, target, sem)
        self.copy.start()
        self.target = target

    def get(self):
        self.copy.wait()
        return self.target


class Stored:
    def __init__(self, ref, target, sem):
        self.ref = ref
        self.copy = pltpu.make_async_copy(ref, target, sem)

    def put(self):
        self.copy.start()


def call(kernel, outs, scratch=(), flops=0, smem=0, far=None, far_out=()):
    far = far or {}

    def run(*args):
        n_in, n_out = len(args), len(outs)
        held = []
        for i in sorted(far):
            rows, width = args[i].shape[-2:]
            if far[i] is not None:
                width = far[i][0]
            held.append(pltpu.VMEM((*args[i].shape[:-2], rows, width), args[i].dtype))
        held += [pltpu.VMEM(*outs[i]) for i in far_out]
        ins = [
            pl.BlockSpec(memory_space=pltpu.SMEM)
            if i < smem
            else pl.BlockSpec(memory_space=pltpu.HBM if i in far else pltpu.VMEM)
            for i in range(n_in)
        ]

        def body(*refs):
            refs = list(refs)
            extra = refs[n_in + n_out :]
            sems = extra[len(held)]
            for k, i in enumerate(sorted(far)):
                source = refs[i]
                if far[i] is not None:
                    width, block = far[i]
                    source = source.at[:, pl.ds(width * block, width)]
                refs[i] = Fetched(source, extra[k], sems.at[k])
            stored = []
            for k, i in enumerate(far_out):
                at = len(far) + k
                stored.append(Stored(extra[at], refs[n_in + i], sems.at[at]))
                refs[n_in + i] = stored[-1]
            kernel(*refs[: n_in + n_out], *extra[len(held) + 1 :])
            for one in stored:
                one.copy.wait()

        return pl.pallas_call(
            body,
            out_shape=[jax.ShapeDtypeStruct(s, d) for s, d in outs],
            in_specs=ins,
            out_specs=[
                pl.BlockSpec(memory_space=pltpu.HBM if i in far_out else pltpu.VMEM)
                for i in range(n_out)
            ],
            scratch_shapes=[*held, pltpu.SemaphoreType.DMA((max(1, len(held)),)), *scratch],
            cost_estimate=pl.CostEstimate(flops=flops, bytes_accessed=1 << 21, transcendentals=0),
            compiler_params=pltpu.CompilerParams(vmem_limit_bytes=24 << 20),
        )(*args)

    return run


def dot(a, b, dims=(((1,), (0,)), ((), ()))):
    return lax.dot_general(a.astype(BF16), b.astype(BF16), dims, preferred_element_type=F32)


def hidden_kernel(place, own, next_, before, across, other, gain, down, up, base, hid, decays):
    x = place[0]
    core = place[1]
    rows = own.shape[0]
    blocks = [own, before, across, next_]
    sums = jnp.zeros((rows, 1), F32)
    for k in range(4):
        mine = blocks[k][...].astype(F32)
        theirs = other[k].astype(F32)
        sums += jnp.sum(mine * mine + theirs * theirs, axis=1, keepdims=True)
    width = own.shape[1]
    scale = lax.rsqrt(sums / (8 * width) + NORM_EPS)
    low = jnp.zeros((rows, down.shape[0]), F32)
    for k in range(4):
        chip = lax.rem(x + k, 4)
        for c, block in ((core, blocks[k][...]), (1 - core, other[k])):
            at = pl.multiple_of((chip * 2 + c) * width, width)
            h = (block.astype(F32) * scale * gain[:, pl.ds(at, width)]).astype(BF16)
            hid.ref[:, pl.ds(at, width)] = h
            low += lax.dot_general(h, down[:, pl.ds(at, width)], NT, preferred_element_type=F32)
    hid.put()
    low = jnp.tanh(low).astype(BF16)
    rate = lax.dot_general(up[...], low, (((0,), (1,)), ((), ())), preferred_element_type=F32)
    heads = base.shape[0]
    base_rows = jnp.concatenate(
        [jnp.broadcast_to(base[h : h + 1, :], (HEAD, rows)) for h in range(heads)], axis=0
    )
    log_decay = jnp.maximum(-jnp.exp(rate + base_rows), DECAY_FLOOR)
    lane = lax.broadcasted_iota(jnp.int32, log_decay.shape, 1) % CHUNK
    total, after = log_decay, log_decay
    step = 1
    while step < CHUNK:
        total = total + jnp.where(lane >= step, pltpu.roll(total, step, 1), 0.0)
        after = after + jnp.where(lane < CHUNK - step, pltpu.roll(after, rows - step, 1), 0.0)
        step *= 2
    decays.ref[0] = total
    decays.ref[1] = total - log_decay
    decays.ref[2] = after - log_decay
    decays.put()


def as_column(row):
    return jnp.broadcast_to(row, (8, row.shape[1])).T[:, :1]


def head_rows(h):
    return slice(h * HEAD, (h + 1) * HEAD)


def band_tables(left, right, start, end, rate, first, heads):
    rows = left.shape[1]
    dist = (
        lax.broadcasted_iota(jnp.int32, (CHUNK, rows), 1) % CHUNK
        - lax.broadcasted_iota(jnp.int32, (CHUNK, rows), 0)
    )
    plain, rated = [], []
    for h in range(heads):
        sl = head_rows(h)
        l, r, s, e = left[sl, :], right[sl, :], start[sl, :], end[sl, :]
        speed = jnp.broadcast_to(rate[sl, :], l.shape)
        t_plain = jnp.zeros((CHUNK, rows), F32)
        t_rated = jnp.zeros((CHUNK, rows), F32)
        for d in range(first, CHUNK):
            rd = r if d == 0 else pltpu.roll(r, d, 1)
            ed = e if d == 0 else pltpu.roll(e, d, 1)
            x = l * rd * jnp.exp(s - ed)
            here = dist == d
            t_plain = jnp.where(here, jnp.sum(x, axis=0, keepdims=True), t_plain)
            t_rated = jnp.where(here, jnp.sum(x * speed, axis=0, keepdims=True), t_rated)
        plain.append(t_plain)
        rated.append(t_rated)
    return plain, rated


def in_chunks(table):
    rows = table.shape[1]
    tall = jnp.concatenate([table] * (rows // CHUNK), axis=0)
    same = (
        lax.broadcasted_iota(jnp.int32, (rows, rows), 0) // CHUNK
        == lax.broadcasted_iota(jnp.int32, (rows, rows), 1) // CHUNK
    )
    return jnp.where(same, tall, 0.0).astype(BF16)


def by_chunk(array):
    rows = array.shape[1]
    chunk = lax.broadcasted_iota(jnp.int32, array.shape, 1) // CHUNK
    return jnp.concatenate(
        [jnp.where(chunk == c, array, 0.0).astype(BF16) for c in range(rows // CHUNK)], axis=0
    )


def state_kernel(hid, w, lr, decays, ends, units, tables, dec):
    rows = dec.shape[0]
    heads = lr.shape[1] // HEAD
    span = heads * HEAD
    lr = as_column(lr[...])
    hid, decays = hid.get(), decays.get()
    kv = jnp.dot(hid[...], w[...], preferred_element_type=F32).astype(BF16).astype(F32)
    kv_t = kv.T
    for h in range(heads):
        k = kv_t[head_rows(h), :]
        square = jnp.sum(k * k, axis=0, keepdims=True) + KEY_EPS
        inv = lax.rsqrt(square)
        units.ref[0, head_rows(h), :] = k * inv
        units.ref[1, head_rows(h), :] = kv_t[span + h * HEAD : span + (h + 1) * HEAD, :] * (square * inv)
    cum_all = decays[0]
    prev = decays[1]
    dec[...] = jnp.exp(cum_all).T
    u = units.ref[0]
    v = units.ref[1]
    plain, rated = band_tables(u, u, prev, cum_all, lr, 1, heads)
    reach = jnp.exp(prev)
    x, q = [], []
    for h in range(heads):
        sl = head_rows(h)
        x.append(jnp.concatenate([-u[sl, :] * reach[sl, :], -dot(v[sl, :], in_chunks(plain[h]))], axis=0))
        q.append(in_chunks(-rated[h]))
    units.put()
    power = 1
    while power < CHUNK:
        for h in range(heads):
            x[h] = x[h] + dot(x[h], q[h])
        power *= 2
        if power < CHUNK:
            for h in range(heads):
                q[h] = dot(q[h], q[h]).astype(BF16)
    left = jnp.exp(decays[2])
    chunks = rows // CHUNK
    grow = []
    for h in range(heads):
        sl = head_rows(h)
        tables.ref[h, :, :rows] = x[h].astype(BF16)
        out_u = u[sl, :] * left[sl, :]
        out_b = out_u * lr[sl, :]
        g = dot(x[h], by_chunk(out_b), NT)
        g_low = g[HEAD:, :] + dot(v[sl, :], by_chunk(out_u), NT)
        grow.append((g[:HEAD, :].astype(BF16), g_low))
    eye = (
        lax.broadcasted_iota(jnp.int32, (2 * HEAD, HEAD), 0)
        == lax.broadcasted_iota(jnp.int32, (2 * HEAD, HEAD), 1)
    ).astype(F32)
    state = [eye] * heads
    zero = jnp.zeros((HEAD, HEAD), F32)
    for c in range(chunks):
        at = slice(c * HEAD, (c + 1) * HEAD)
        last = c * CHUNK + CHUNK - 1
        for h in range(heads):
            low = state[h].astype(BF16)
            tables.ref[h, :, rows + c * HEAD : rows + (c + 1) * HEAD] = low
            kept = state[h] * dec[last : last + 1, head_rows(h)]
            added = jnp.concatenate([zero, grow[h][1][:, at]], axis=0)
            state[h] = kept + added + jnp.dot(low, grow[h][0][:, at], preferred_element_type=F32)
    packed = jnp.concatenate(state, axis=1).astype(BF16)
    for k in range(ends.shape[0]):
        ends[k] = packed
    tables.put()


def read_kernel(hid, w, lr, decays, units, tables, out):
    heads = lr.shape[1] // HEAD
    lr = as_column(lr[...])
    hid, w, decays, units = hid.get(), w.get(), decays.get(), units.get()
    rows = hid.shape[0]
    reads = jnp.dot(hid[...], w[...], preferred_element_type=F32).astype(BF16).astype(F32)
    r = reads.T
    cum_all = decays[0]
    plain, rated = band_tables(r, units[0], cum_all, cum_all, lr, 0, heads)
    reach = r * jnp.exp(cum_all)
    tables = tables.get()
    for h in range(heads):
        sl = head_rows(h)
        mixed = dot(tables[h, :, :rows], in_chunks(rated[h]))
        query = mixed[:HEAD, :] + reach[sl, :]
        local = mixed[HEAD:, :] + dot(units[1, sl, :], in_chunks(plain[h]))
        both = dot(tables[h, :, rows:], by_chunk(query))
        out.ref[h, :HEAD, :] = both[:HEAD, :]
        out.ref[h, HEAD:, :] = both[HEAD:, :] + local
    out.put()


def chain(earlier, later):
    moved = jnp.dot(earlier.astype(BF16), later[:HEAD, :], preferred_element_type=F32)
    return moved + jnp.concatenate([jnp.zeros((HEAD, HEAD), F32), later[HEAD:, :].astype(F32)], axis=0)


def row_kernel(place, pieces, total_out, inside_out):
    devices, heads = pieces.shape[0], pieces.shape[2] // HEAD
    eye = (
        lax.broadcasted_iota(jnp.int32, (2 * HEAD, HEAD), 0)
        == lax.broadcasted_iota(jnp.int32, (2 * HEAD, HEAD), 1)
    ).astype(F32)
    total = [eye] * heads
    inside = [eye] * heads
    for k in range(devices):
        passed = k < place[0]
        for h in range(heads):
            later = pieces[k, :, head_rows(h)]
            total[h] = later.astype(F32) if k == 0 else chain(total[h], later)
            inside[h] = jnp.where(passed, total[h], inside[h])
    packed = jnp.concatenate(total, axis=1).astype(BF16)
    for k in range(total_out.shape[0]):
        total_out[k] = packed
    inside_out[...] = jnp.concatenate(inside, axis=1).astype(BF16)


def final_kernel(place, pieces, inside, local, gain, att, w, out):
    devices, heads = pieces.shape[0], pieces.shape[2] // HEAD
    state = [jnp.zeros((HEAD, HEAD), F32)] * heads
    for k in range(devices - 1):
        passed = k < place[0]
        for h in range(heads):
            later = pieces[k, :, head_rows(h)]
            new = jnp.dot(state[h].astype(BF16), later[:HEAD, :], preferred_element_type=F32)
            state[h] = jnp.where(passed, new + later[HEAD:, :].astype(F32), state[h])
    rows = []
    gain = as_column(gain[...])
    inside, local = inside.get(), local.get()
    for h in range(heads):
        near = inside[:, head_rows(h)]
        start = jnp.dot(state[h].astype(BF16), near[:HEAD, :], preferred_element_type=F32)
        start = start + near[HEAD:, :].astype(F32)
        y = dot(start, local[h, :HEAD, :]) + local[h, HEAD:, :]
        centered = y - jnp.mean(y, axis=0, keepdims=True)
        variance = jnp.mean(centered * centered, axis=0, keepdims=True)
        rows.append(centered * lax.rsqrt(variance + GROUP_EPS) * gain[head_rows(h), :])
    rec = jnp.concatenate(rows, axis=0).T.astype(BF16)
    mix = jnp.concatenate([att.get()[...], rec], axis=1)
    w = w.get()
    groups, width = out.shape[0], 512
    size = out.shape[1]
    for n in range(w.shape[0] // width):
        at = slice(n * width, (n + 1) * width)
        part = lax.dot_general(mix, w[at, :], NT, preferred_element_type=F32).astype(BF16)
        for g in range(groups):
            out[g, :, at] = part[g * size : (g + 1) * size, :]


def head_rms(values, gain):
    heads = []
    for h in range(values.shape[1] // HEAD):
        x = values[:, head_rows(h)]
        mean_sq = jnp.mean(x * x, axis=1, keepdims=True)
        heads.append((x * lax.rsqrt(mean_sq + NORM_EPS) * gain).astype(BF16))
    return heads


def attention_in_kernel(hid, w, query_gain, key_gain, queries, keys_values):
    q_w, kv_w = queries.shape[1], keys_values.shape[1] // 2
    hid, w = hid.get(), w.get()
    rows = jnp.dot(hid[...], w[...], preferred_element_type=F32).astype(BF16)
    normed = head_rms(rows[:, :q_w].astype(F32), query_gain[...])
    queries[...] = jnp.concatenate(normed, axis=1)
    normed = head_rms(rows[:, q_w : q_w + kv_w].astype(F32), key_gain[...])
    keys_values[...] = jnp.concatenate(normed + [rows[:, q_w + kv_w :]], axis=1)


def attention_kernel(place, sink, queries, keys_values, before, out, lse):
    rows = queries.shape[0]
    heads = queries.shape[1] // HEAD
    shape = (2 * WINDOW, WINDOW)
    key_at = lax.broadcasted_iota(jnp.int32, shape, 0)
    lag = lax.broadcasted_iota(jnp.int32, shape, 1) + WINDOW - key_at
    near = (lag >= 0) & (lag < WINDOW)
    for n in range(rows // WINDOW):
        at = slice(n * WINDOW, (n + 1) * WINDOW)
        if n == 0:
            band = jnp.concatenate([before[...], keys_values[at, :]], axis=0)
            allowed = near & ((key_at >= WINDOW) | (place[0] > 0))
        else:
            band = keys_values[(n - 1) * WINDOW : (n + 1) * WINDOW, :]
            allowed = near
        tiles = []
        for h in range(heads):
            score = lax.dot_general(
                band[:, :HEAD], queries[at, head_rows(h)], NT, preferred_element_type=F32
            ) * (1.0 / math.sqrt(HEAD))
            score = jnp.where(allowed, score, -jnp.inf)
            top = jnp.maximum(jnp.max(score, axis=0, keepdims=True), sink[h])
            weight = jnp.exp(score - top)
            total = jnp.sum(weight, axis=0, keepdims=True) + jnp.exp(sink[h] - top)
            lse[h : h + 1, at] = top + jnp.log(total)
            probs = (weight / total).astype(BF16)
            mixed = lax.dot_general(probs, band[:, HEAD:], TN, preferred_element_type=F32)
            tiles.append(mixed.astype(BF16))
        out[at, :] = jnp.concatenate(tiles, axis=1)


def per_device(
    tokens,
    norm_gain,
    query_w,
    key_w,
    value_w,
    recept_w,
    rec_key_w,
    rec_value_w,
    decay_down,
    decay_up,
    decay_base,
    learn_rate,
    query_gain,
    key_gain,
    sink_logit,
    group_gain,
    out_att_w,
    out_rec_w,
):
    rows = tokens.shape[0]
    span = recept_w.shape[1]
    heads = span // HEAD
    features = norm_gain.shape[0]
    groups = lax.axis_size(("fs", "tp"))
    place_zy = [lax.axis_index(a).astype(jnp.int32).reshape(1) for a in SP]

    own = jnp.concatenate(
        [rec_key_w, rec_value_w, query_w, key_w, value_w, out_att_w.T, out_rec_w.T, recept_w], axis=1
    )
    column = from_everyone(own, "sp_1").reshape(-1, own.shape[1])
    state_w = from_everyone(column[:, : 2 * span], "sp_0").reshape(features, 2 * span)
    before = ring_shift(tokens, "fs", -1)
    across = ring_shift(tokens, "fs", 2)
    next_ = ring_shift(tokens, "fs", 1)
    other = ring_shift(jnp.stack([tokens, before, across, next_]), "tp", 1)


    place_xc = jnp.stack([lax.axis_index("fs"), lax.axis_index("tp")]).astype(jnp.int32)
    decay_cols = lax.dynamic_slice_in_dim(
        decay_up, lax.axis_index(("fs", "tp")) * span, span, 1
    )
    flat = (span, rows)
    hid, decays = call(
        hidden_kernel,
        [((rows, features), BF16), ((3, *flat), F32)],
        smem=1,
        flops=1 << 27,
        far_out=(0, 1),
    )(
        place_xc, tokens, next_, before, across, other, norm_gain.reshape(1, -1), decay_down.T, decay_cols, decay_base
    )

    held, hid = lax.optimization_barrier((column[:, 2 * span :], hid))
    other_w = lax.all_gather(held, "sp_0", axis=0, tiled=True)

    lr = learn_rate.reshape(1, span)
    chunks = rows // CHUNK
    pair = (2 * HEAD, span)
    ends, units, tables = call(
        state_kernel,
        [
            ((lax.axis_size("sp_1"), *pair), BF16),
            ((2, *flat), F32),
            ((heads, 2 * HEAD, rows + chunks * HEAD), BF16),
        ],
        scratch=[pltpu.VMEM((rows, span), F32)],
        flops=1 << 31,
        far={0: None, 3: None},
        far_out=(1, 2),
    )(hid, state_w, lr, decays)

    row_pieces = lax.all_to_all(ends, "sp_1", 0, 0, tiled=True)
    row_total, inside = call(
        row_kernel, [((lax.axis_size("sp_0"), *pair), BF16), (pair, BF16)], smem=1, flops=1 << 27
    )(place_zy[1], row_pieces)
    all_pieces = lax.all_to_all(row_total, "sp_0", 0, 0, tiled=True)

    q_w, kv_w = query_w.shape[1], key_w.shape[1]
    whole = q_w + 2 * kv_w
    (local,) = call(
        read_kernel, [((heads, 2 * HEAD, rows), F32)], flops=1 << 31,
        far={0: None, 1: (span, 2 * whole // span), 3: None, 4: None, 5: None}, far_out=(0,),
    )(hid, other_w, lr, decays, units, tables)
    queries, keys_values = call(
        attention_in_kernel,
        [((rows, q_w), BF16), ((rows, 2 * kv_w), BF16)],
        flops=1 << 28,
        far={0: None, 1: (whole, 0)},
    )(hid, other_w, query_gain.reshape(1, HEAD), key_gain.reshape(1, HEAD))
    before_keys = passed_along(keys_values[rows - WINDOW :], SP, 1)
    place_sp = lax.axis_index(SP).astype(jnp.int32).reshape(1)
    att_mix, row_lse = call(
        attention_kernel, [((rows, q_w), BF16), ((q_w // HEAD, rows), F32)], smem=2, flops=1 << 28
    )(place_sp, sink_logit, queries, keys_values, before_keys)

    (partial,) = call(
        final_kernel,
        [((groups, rows // groups, features), BF16)],
        smem=1,
        flops=1 << 30,
        far={2: None, 3: None, 5: None, 6: (whole, 1)},
    )(place_zy[0], all_pieces, inside, local, group_gain.reshape(1, span), att_mix, other_w)
    tiles = lax.all_to_all(partial, ("fs", "tp"), 0, 0, tiled=True)
    mixed = jnp.sum(tiles.astype(F32), axis=0).astype(BF16)
    return (mixed, row_lse)


def solution(mesh):
    split = Mesh(
        mesh.devices.reshape(8, 8, mesh.shape["fs"], mesh.shape["tp"]), ("sp_0", "sp_1", "fs", "tp")
    )
    in_specs = (
        P(SP, ("fs", "tp")),
        P(),
        P(SP, ("fs", "tp")),
        P(SP, ("fs", "tp")),
        P(SP, ("fs", "tp")),
        P(SP, ("fs", "tp")),
        P(SP, ("fs", "tp")),
        P(SP, ("fs", "tp")),
        P(),
        P(),
        P(("fs", "tp"), SP),
        P(("fs", "tp")),
        P(),
        P(),
        P(("fs", "tp")),
        P(("fs", "tp")),
        P(("fs", "tp"), SP),
        P(("fs", "tp"), SP),
    )
    out_specs = (P(SP_FS_TP, None), P(("fs", "tp"), SP))

    return jax.shard_map(
        per_device, mesh=split, in_specs=in_specs, out_specs=out_specs, check_vma=False
    )
```

```python
import math

import jax
import jax.numpy as jnp
from jax import lax
from jax.experimental import pallas as pl
from jax.experimental.pallas import tpu as pltpu
from jax.sharding import Mesh
from jax.sharding import PartitionSpec as P

HEAD = 64
WINDOW = 128
CHUNK = 32
HALF = 16
SP = ("sp_0", "sp_1")
SP_FS_TP = ("sp_0", "sp_1", "fs", "tp")
F32 = jnp.float32
BF16 = jnp.bfloat16

NORM_EPS = 1e-06
KEY_EPS = 1e-06
GROUP_EPS = 0.00064
DECAY_FLOOR = -104.0

NT = (((1,), (1,)), ((), ()))
TN = (((0,), (0,)), ((), ()))


def ring_shift(array, axis, by):
    devices = lax.axis_size(axis)
    return lax.ppermute(array, axis, [(i, (i + by) % devices) for i in range(devices)])


def passed_along(array, axis, by):
    devices = lax.axis_size(axis)
    pairs = [(i, i + by) for i in range(devices) if 0 <= i + by < devices]
    return lax.ppermute(array, axis, pairs)


def from_everyone(array, axis):
    copies = jnp.broadcast_to(array, (lax.axis_size(axis), *array.shape))
    return lax.all_to_all(copies, axis, split_axis=0, concat_axis=0, tiled=True)


class Fetched:
    def __init__(self, source, target, sem):
        self.copy = pltpu.make_async_copy(source, target, sem)
        self.copy.start()
        self.target = target

    def get(self):
        self.copy.wait()
        return self.target


class Stored:
    def __init__(self, ref, target, sem):
        self.ref = ref
        self.copy = pltpu.make_async_copy(ref, target, sem)

    def put(self):
        self.copy.start()


def call(kernel, outs, scratch=(), flops=0, smem=0, far=None, far_out=()):
    far = far or {}

    def run(*args):
        n_in, n_out = len(args), len(outs)
        held = []
        for i in sorted(far):
            rows, width = args[i].shape[-2:]
            if far[i] is not None:
                _, rows, _, width = far[i]
            held.append(pltpu.VMEM((*args[i].shape[:-2], rows, width), args[i].dtype))
        held += [pltpu.VMEM(*outs[i]) for i in far_out]
        ins = [
            pl.BlockSpec(memory_space=pltpu.SMEM)
            if i < smem
            else pl.BlockSpec(memory_space=pltpu.HBM if i in far else pltpu.VMEM)
            for i in range(n_in)
        ]

        def body(*refs):
            refs = list(refs)
            extra = refs[n_in + n_out :]
            sems = extra[len(held)]
            for k, i in enumerate(sorted(far)):
                source = refs[i]
                if far[i] is not None:
                    source = source.at[pl.ds(*far[i][:2]), pl.ds(*far[i][2:])]
                refs[i] = Fetched(source, extra[k], sems.at[k])
            stored = []
            for k, i in enumerate(far_out):
                at = len(far) + k
                stored.append(Stored(extra[at], refs[n_in + i], sems.at[at]))
                refs[n_in + i] = stored[-1]
            kernel(*refs[: n_in + n_out], *extra[len(held) + 1 :])
            for one in stored:
                one.copy.wait()

        args = [
            pltpu.with_memory_space_constraint(a, pltpu.HBM) if i in far else a
            for i, a in enumerate(args)
        ]
        return pl.pallas_call(
            body,
            out_shape=[
                pltpu.HBM(*o) if i in far_out else jax.ShapeDtypeStruct(*o)
                for i, o in enumerate(outs)
            ],
            in_specs=ins,
            out_specs=[
                pl.BlockSpec(memory_space=pltpu.HBM if i in far_out else pltpu.VMEM)
                for i in range(n_out)
            ],
            scratch_shapes=[*held, pltpu.SemaphoreType.DMA((max(1, len(held)),)), *scratch],
            cost_estimate=pl.CostEstimate(flops=flops, bytes_accessed=1 << 21, transcendentals=0),
            compiler_params=pltpu.CompilerParams(vmem_limit_bytes=24 << 20),
        )(*args)

    return run


def dot(a, b, dims=(((1,), (0,)), ((), ()))):
    return lax.dot_general(a.astype(BF16), b.astype(BF16), dims, preferred_element_type=F32)


def running_sums(x, size):
    rows = x.shape[1]
    lane = lax.broadcasted_iota(jnp.int32, x.shape, 1) % size
    total, after = x, x
    step = 1
    while step < size:
        total = total + jnp.where(lane >= step, pltpu.roll(total, step, 1), 0.0)
        after = after + jnp.where(lane < size - step, pltpu.roll(after, rows - step, 1), 0.0)
        step *= 2
    return total, after


def hidden_kernel(place, own, next_, before, across, other, gain, down, up, base, hid, decays):
    x = place[0]
    core = place[1]
    rows = own.shape[0]
    blocks = [own, before, across, next_]
    sums = jnp.zeros((rows, 1), F32)
    for k in range(4):
        mine = blocks[k][...].astype(F32)
        theirs = other[k].astype(F32)
        sums += jnp.sum(mine * mine + theirs * theirs, axis=1, keepdims=True)
    width = own.shape[1]
    scale = lax.rsqrt(sums / (8 * width) + NORM_EPS)
    low = jnp.zeros((rows, down.shape[0]), F32)
    for k in range(4):
        chip = lax.rem(x + k, 4)
        for c, block in ((core, blocks[k][...]), (1 - core, other[k])):
            at = pl.multiple_of((chip * 2 + c) * width, width)
            h = (block.astype(F32) * scale * gain[:, pl.ds(at, width)]).astype(BF16)
            hid.ref[:, pl.ds(at, width)] = h
            low += lax.dot_general(h, down[:, pl.ds(at, width)], NT, preferred_element_type=F32)
    hid.put()
    low = jnp.tanh(low[WINDOW:, :]).astype(BF16)
    rate = lax.dot_general(up[...], low, (((0,), (1,)), ((), ())), preferred_element_type=F32)
    heads = base.shape[0]
    base_rows = jnp.concatenate(
        [jnp.broadcast_to(base[h : h + 1, :], (HEAD, base.shape[1])) for h in range(heads)], axis=0
    )
    log_decay = jnp.maximum(-jnp.exp(rate + base_rows), DECAY_FLOOR)
    for k, size in enumerate((CHUNK, HALF)):
        total, after = running_sums(log_decay, size)
        decays.ref[3 * k] = total
        decays.ref[3 * k + 1] = total - log_decay
        decays.ref[3 * k + 2] = after - log_decay
    decays.put()


def as_column(row):
    return jnp.broadcast_to(row, (8, row.shape[1])).T[:, :1]


def head_rows(h):
    return slice(h * HEAD, (h + 1) * HEAD)


def pair_tables(left, right, start, end, near_start, near_end, rate, first, heads):
    rows = left.shape[1]
    at_j = lax.broadcasted_iota(jnp.int32, (CHUNK, rows), 0)
    at_i = lax.broadcasted_iota(jnp.int32, (CHUNK, rows), 1) % CHUNK
    dist = jnp.where(at_i // HALF == at_j // HALF, at_i - at_j, -1)
    all_j = lax.broadcasted_iota(jnp.int32, (rows, rows), 0)
    all_i = lax.broadcasted_iota(jnp.int32, (rows, rows), 1)
    same = all_i // CHUNK == all_j // CHUNK
    across = same & (all_i // HALF > all_j // HALF)
    plain, rated = [], []
    for h in range(heads):
        sl = head_rows(h)
        l, r, s, e = left[sl, :], right[sl, :], start[sl, :], end[sl, :]
        speed = jnp.broadcast_to(rate[sl, :], l.shape)
        t_plain = jnp.zeros((CHUNK, rows), F32)
        t_rated = jnp.zeros((CHUNK, rows), F32)
        for d in range(first, HALF):
            rd = r if d == 0 else pltpu.roll(r, d, 1)
            ed = e if d == 0 else pltpu.roll(e, d, 1)
            x = l * rd * jnp.exp(s - ed)
            here = dist == d
            t_plain = jnp.where(here, jnp.sum(x, axis=0, keepdims=True), t_plain)
            t_rated = jnp.where(here, jnp.sum(x * speed, axis=0, keepdims=True), t_rated)
        later = l * jnp.exp(near_start[sl, :])
        earlier = r * jnp.exp(near_end[sl, :])
        for table, weight, out in ((t_plain, earlier, plain), (t_rated, earlier * speed, rated)):
            far = dot(weight, later, TN)
            tall = jnp.concatenate([table] * (rows // CHUNK), axis=0)
            out.append(jnp.where(across, far, jnp.where(same, tall, 0.0)).astype(BF16))
    return plain, rated


def by_chunk(array):
    rows = array.shape[1]
    chunk = lax.broadcasted_iota(jnp.int32, array.shape, 1) // CHUNK
    return jnp.concatenate(
        [jnp.where(chunk == c, array, 0.0).astype(BF16) for c in range(rows // CHUNK)], axis=0
    )


def spread(row):
    eye = (
        lax.broadcasted_iota(jnp.int32, (HEAD, HEAD), 0)
        == lax.broadcasted_iota(jnp.int32, (HEAD, HEAD), 1)
    )
    return jnp.where(eye, row, 0.0)


def followed(state, kept, change, added):
    low = state.astype(BF16)
    new = state * kept + jnp.dot(low, change.astype(BF16), preferred_element_type=F32)
    return new + jnp.concatenate([jnp.zeros((HEAD, HEAD), F32), added], axis=0)


def kept_by(decays, c, h):
    last = c * CHUNK + CHUNK - 1
    return decays[last : last + 1, head_rows(h)]


def state_kernel(hid, w, lr, decays, ends, units, tables, changes, adds, dec):
    rows = dec.shape[0]
    lr = as_column(lr.get()[...])
    span = lr.shape[0]
    heads = span // HEAD
    hid, decays = hid.get(), decays.get()
    kv = jnp.dot(hid[...], w[...], preferred_element_type=F32).astype(BF16).astype(F32)
    kv_t = kv.T
    for h in range(heads):
        k = kv_t[head_rows(h), :]
        square = jnp.sum(k * k, axis=0, keepdims=True) + KEY_EPS
        inv = lax.rsqrt(square)
        units.ref[0, head_rows(h), :] = k * inv
        units.ref[1, head_rows(h), :] = kv_t[span + h * HEAD : span + (h + 1) * HEAD, :] * (square * inv)
    cum, prev = decays[0], decays[1]
    dec[...] = jnp.exp(cum).T
    u = units.ref[0]
    v = units.ref[1]
    plain, rated = pair_tables(u, u, prev, cum, decays[4], decays[5], lr, 1, heads)
    reach = jnp.exp(prev)
    x, q = [], []
    for h in range(heads):
        sl = head_rows(h)
        x.append(jnp.concatenate([-u[sl, :] * reach[sl, :], -dot(v[sl, :], plain[h])], axis=0))
        q.append(-rated[h])
    units.put()
    power = 1
    while power < CHUNK:
        for h in range(heads):
            x[h] = x[h] + dot(x[h], q[h])
        power *= 2
        if power < CHUNK:
            for h in range(heads):
                q[h] = dot(q[h], q[h]).astype(BF16)
    left = jnp.exp(decays[2])
    chunks = rows // CHUNK
    for h in range(heads):
        sl = head_rows(h)
        tables.ref[h] = x[h].astype(BF16)
        out_u = u[sl, :] * left[sl, :]
        out_b = out_u * lr[sl, :]
        g = dot(x[h], by_chunk(out_b), NT)
        changes.ref[h] = g[:HEAD, :].astype(BF16)
        adds.ref[h] = g[HEAD:, :] + dot(v[sl, :], by_chunk(out_u), NT)
    parts = []
    for h in range(heads):
        for c in range(chunks):
            at = slice(c * HEAD, (c + 1) * HEAD)
            parts.append((h, kept_by(dec, c, h), changes.ref[h, :, at].astype(F32), adds.ref[h, :, at]))
    tables.put()
    changes.put()
    adds.put()
    while len(parts) > heads:
        joined = []
        for (h, kept, change, added), (_, kept2, change2, added2) in zip(parts[::2], parts[1::2]):
            both = jnp.concatenate([change + spread(kept), added], axis=0)
            both = followed(both, kept2, change2, added2)
            kept = kept * kept2
            joined.append((h, kept, both[:HEAD, :] - spread(kept), both[HEAD:, :]))
        parts = joined
    packed = jnp.concatenate(
        [jnp.concatenate([change + spread(kept), added], axis=0) for _, kept, change, added in parts],
        axis=1,
    ).astype(BF16)
    for k in range(ends.shape[0]):
        ends[k] = packed


def read_part(reads, lr, decays, units, tables, changes, adds, out):
    rows = reads.shape[0]
    heads = lr.shape[0] // HEAD
    r = reads.T
    cum = decays[0]
    reach = jnp.exp(cum)
    dec = reach.T
    eye = jnp.concatenate([spread(jnp.ones((1, HEAD), F32)), jnp.zeros((HEAD, HEAD), F32)], axis=0)
    starts = [[eye] for _ in range(heads)]
    for c in range(rows // CHUNK - 1):
        at = slice(c * HEAD, (c + 1) * HEAD)
        for h in range(heads):
            starts[h].append(
                followed(starts[h][-1], kept_by(dec, c, h), changes[h, :, at], adds[h, :, at])
            )
    near = decays[3]
    plain, rated = pair_tables(r, units[0], cum, cum, near, decays[5], lr, 0, heads)
    reach = r * reach
    for h in range(heads):
        sl = head_rows(h)
        mixed = dot(tables[h], rated[h])
        query = mixed[:HEAD, :] + reach[sl, :]
        local = mixed[HEAD:, :] + dot(units[1, sl, :], plain[h])
        start = jnp.concatenate([x.astype(BF16) for x in starts[h]], axis=1)
        both = dot(start, by_chunk(query))
        out.ref[h, :HEAD, :] = both[:HEAD, :]
        out.ref[h, HEAD:, :] = both[HEAD:, :] + local
    out.put()


def chain(earlier, later):
    moved = jnp.dot(earlier.astype(BF16), later[:HEAD, :], preferred_element_type=F32)
    return moved + jnp.concatenate([jnp.zeros((HEAD, HEAD), F32), later[HEAD:, :].astype(F32)], axis=0)


def row_kernel(place, pieces, total_out, inside_out):
    devices, heads = pieces.shape[0], pieces.shape[2] // HEAD
    eye = (
        lax.broadcasted_iota(jnp.int32, (2 * HEAD, HEAD), 0)
        == lax.broadcasted_iota(jnp.int32, (2 * HEAD, HEAD), 1)
    ).astype(F32)
    total = [eye] * heads
    inside = [eye] * heads
    for k in range(devices):
        passed = k < place[0]
        for h in range(heads):
            later = pieces[k, :, head_rows(h)]
            total[h] = later.astype(F32) if k == 0 else chain(total[h], later)
            inside[h] = jnp.where(passed, total[h], inside[h])
    packed = jnp.concatenate(total, axis=1).astype(BF16)
    for k in range(total_out.shape[0]):
        total_out[k] = packed
    inside_out[...] = jnp.concatenate(inside, axis=1).astype(BF16)


def final_kernel(place, pieces, inside, local, gain, att, w, out):
    devices, heads = pieces.shape[0], pieces.shape[2] // HEAD
    state = [jnp.zeros((HEAD, HEAD), F32)] * heads
    for k in range(devices - 1):
        passed = k < place[0]
        for h in range(heads):
            later = pieces[k, :, head_rows(h)]
            new = jnp.dot(state[h].astype(BF16), later[:HEAD, :], preferred_element_type=F32)
            state[h] = jnp.where(passed, new + later[HEAD:, :].astype(F32), state[h])
    rows = []
    gain = as_column(gain.get()[...])
    inside, local = inside.get(), local.get()
    for h in range(heads):
        near = inside[:, head_rows(h)]
        start = jnp.dot(state[h].astype(BF16), near[:HEAD, :], preferred_element_type=F32)
        start = start + near[HEAD:, :].astype(F32)
        y = dot(start, local[h, :HEAD, :]) + local[h, HEAD:, :]
        centered = y - jnp.mean(y, axis=0, keepdims=True)
        variance = jnp.mean(centered * centered, axis=0, keepdims=True)
        rows.append(centered * lax.rsqrt(variance + GROUP_EPS) * gain[head_rows(h), :])
    rec = jnp.concatenate(rows, axis=0).T.astype(BF16)
    mix = jnp.concatenate([att.get()[...], rec], axis=1)
    w = w.get()
    groups, width = out.shape[0], 512
    size = out.shape[1]
    for n in range(w.shape[0] // width):
        at = slice(n * width, (n + 1) * width)
        part = lax.dot_general(mix, w[at, :], NT, preferred_element_type=F32).astype(BF16)
        for g in range(groups):
            out[g % 2 * (groups // 2) + g // 2, :, at] = part[g * size : (g + 1) * size, :]


def head_rms(values, gain):
    heads = []
    for h in range(values.shape[1] // HEAD):
        x = values[:, head_rows(h)]
        mean_sq = jnp.mean(x * x, axis=1, keepdims=True)
        heads.append((x * lax.rsqrt(mean_sq + NORM_EPS) * gain).astype(BF16))
    return heads


def attention_part(at_start, sink, queries, keys, values, out, lse):
    shape = (2 * WINDOW, WINDOW)
    key_at = lax.broadcasted_iota(jnp.int32, shape, 0)
    lag = lax.broadcasted_iota(jnp.int32, shape, 1) + WINDOW - key_at
    near = (lag >= 0) & (lag < WINDOW)
    for n in range(queries[0].shape[0] // WINDOW):
        at = slice(n * WINDOW, (n + 1) * WINDOW)
        band = slice(n * WINDOW, (n + 2) * WINDOW)
        allowed = near & ((key_at >= WINDOW) | jnp.logical_not(at_start)) if n == 0 else near
        tiles = []
        for h, query in enumerate(queries):
            score = lax.dot_general(
                keys[band, :], query[at, :], NT, preferred_element_type=F32
            ) * (1.0 / math.sqrt(HEAD))
            score = jnp.where(allowed, score, -jnp.inf)
            top = jnp.maximum(jnp.max(score, axis=0, keepdims=True), sink[h])
            weight = jnp.exp(score - top)
            total = jnp.sum(weight, axis=0, keepdims=True) + jnp.exp(sink[h] - top)
            lse[h : h + 1, at] = top + jnp.log(total)
            probs = (weight / total).astype(BF16)
            mixed = lax.dot_general(probs, values[band, :], TN, preferred_element_type=F32)
            tiles.append(mixed.astype(BF16))
        out.ref[at, :] = jnp.concatenate(tiles, axis=1)
    out.put()


def late_kernel(place, sink, hid, w, query_gain, key_gain, lr, decays, units, tables, changes, adds, local, mix, lse):
    q_w = mix.ref.shape[1]
    lr = as_column(lr.get()[...])
    hid, w = hid.get(), w.get()
    both = jnp.dot(hid[...], w[...], preferred_element_type=F32).astype(BF16)
    own = both[WINDOW:, :]
    whole = own.shape[1] - lr.shape[0]
    made = [ref.get() for ref in (decays, units, tables, changes, adds)]
    read_part(own[:, whole:].astype(F32), lr, *made, local)
    queries = head_rms(own[:, :q_w].astype(F32), query_gain[...])
    (keys,) = head_rms(both[:, q_w : q_w + HEAD].astype(F32), key_gain[...])
    attention_part(place[0] == 0, sink, queries, keys, both[:, q_w + HEAD : whole], mix, lse)


def per_device(
    tokens,
    norm_gain,
    query_w,
    key_w,
    value_w,
    recept_w,
    rec_key_w,
    rec_value_w,
    decay_down,
    decay_up,
    decay_base,
    learn_rate,
    query_gain,
    key_gain,
    sink_logit,
    group_gain,
    out_att_w,
    out_rec_w,
):
    rows = tokens.shape[0]
    span = recept_w.shape[1]
    heads = span // HEAD
    features = norm_gain.shape[0]
    groups = lax.axis_size(("fs", "tp"))
    place_zy = [lax.axis_index(a).astype(jnp.int32).reshape(1) for a in SP]

    own = jnp.concatenate(
        [rec_key_w, rec_value_w, query_w, key_w, value_w, recept_w, out_att_w.T, out_rec_w.T], axis=1
    )
    column = from_everyone(own, "sp_1").reshape(-1, own.shape[1])
    state_w = from_everyone(column[:, : 2 * span], "sp_0").reshape(features, 2 * span)
    ahead = passed_along(tokens[rows - WINDOW :], SP, 1)
    tokens = jnp.concatenate([ahead, tokens], axis=0)
    before = ring_shift(tokens, "fs", -1)
    across = ring_shift(tokens, "fs", 2)
    next_ = ring_shift(tokens, "fs", 1)
    held, before = lax.optimization_barrier((column[:, 2 * span :], before))
    other_w = lax.all_gather(held, "sp_0", axis=0, tiled=True)
    other = ring_shift(jnp.stack([tokens, before, across, next_]), "tp", 1)


    place_xc = jnp.stack([lax.axis_index("fs"), lax.axis_index("tp")]).astype(jnp.int32)
    decay_cols = lax.dynamic_slice_in_dim(
        decay_up, lax.axis_index(("fs", "tp")) * span, span, 1
    )
    flat = (span, rows)
    hid, decays = call(
        hidden_kernel, [((WINDOW + rows, features), BF16), ((6, *flat), F32)], smem=1, flops=1 << 27, far_out=(0, 1)
    )(
        place_xc, tokens, next_, before, across, other, norm_gain.reshape(1, -1), decay_down.T, decay_cols, decay_base
    )


    lr = learn_rate.reshape(1, span)
    chunks = rows // CHUNK
    pair = (2 * HEAD, span)
    ends, *made = call(
        state_kernel,
        [
            ((lax.axis_size("sp_1"), *pair), BF16),
            ((2, *flat), F32),
            ((heads, 2 * HEAD, rows), BF16),
            ((heads, HEAD, chunks * HEAD), BF16),
            ((heads, HEAD, chunks * HEAD), F32),
        ],
        scratch=[pltpu.VMEM((rows, span), F32)],
        flops=1 << 31,
        far={0: (WINDOW, rows, 0, features), 2: None, 3: None},
        far_out=(1, 2, 3, 4),
    )(hid, state_w, lr, decays)

    row_pieces = lax.all_to_all(ends, "sp_1", 0, 0, tiled=True)
    row_total, inside = call(
        row_kernel, [((lax.axis_size("sp_0"), *pair), BF16), (pair, BF16)], smem=1, flops=1 << 27
    )(place_zy[1], row_pieces)
    all_pieces = lax.all_to_all(row_total, "sp_0", 0, 0, tiled=True)

    q_w, kv_w = query_w.shape[1], key_w.shape[1]
    early = q_w + 2 * kv_w + span
    place_sp = lax.axis_index(SP).astype(jnp.int32).reshape(1)
    local, att_mix, row_lse = call(
        late_kernel,
        [((heads, 2 * HEAD, rows), F32), ((rows, q_w), BF16), ((q_w // HEAD, rows), F32)],
        smem=2,
        flops=1 << 31,
        far={2: None, 3: (0, features, 0, early), **{i: None for i in range(6, 12)}},
        far_out=(0, 1),
    )(
        place_sp, sink_logit, hid, other_w, query_gain.reshape(1, HEAD), key_gain.reshape(1, HEAD),
        lr, decays, *made,
    )

    (partial,) = call(
        final_kernel,
        [((groups, rows // groups, features), BF16)],
        smem=1,
        flops=1 << 30,
        far={2: None, 3: None, 4: None, 5: None, 6: (0, features, early, q_w + span)},
    )(place_zy[0], all_pieces, inside, local, group_gain.reshape(1, span), att_mix, other_w)
    tiles = lax.all_to_all(partial, "tp", 0, 0, tiled=True).reshape(2, groups // 2, -1, features)
    tiles = jnp.sum(tiles.astype(F32), axis=0).astype(BF16)
    tiles = lax.all_to_all(tiles, "fs", 0, 0, tiled=True)
    mixed = jnp.sum(tiles.astype(F32), axis=0).astype(BF16)
    return (mixed, row_lse)


def solution(mesh):
    split = Mesh(
        mesh.devices.reshape(8, 8, mesh.shape["fs"], mesh.shape["tp"]), ("sp_0", "sp_1", "fs", "tp")
    )
    in_specs = (
        P(SP, ("fs", "tp")),
        P(),
        P(SP, ("fs", "tp")),
        P(SP, ("fs", "tp")),
        P(SP, ("fs", "tp")),
        P(SP, ("fs", "tp")),
        P(SP, ("fs", "tp")),
        P(SP, ("fs", "tp")),
        P(),
        P(),
        P(("fs", "tp"), SP),
        P(("fs", "tp")),
        P(),
        P(),
        P(("fs", "tp")),
        P(("fs", "tp")),
        P(("fs", "tp"), SP),
        P(("fs", "tp"), SP),
    )
    out_specs = (P(SP_FS_TP, None), P(("fs", "tp"), SP))

    return jax.shard_map(per_device, mesh=split, in_specs=in_specs, out_specs=out_specs, check_vma=False)
```

```python
import math

import jax
import jax.numpy as jnp
from jax import lax
from jax.experimental import pallas as pl
from jax.experimental.pallas import tpu as pltpu
from jax.sharding import Mesh
from jax.sharding import PartitionSpec as P

HEAD = 64
WINDOW = 128
CHUNK = 32
HALF = 16
SP = ("sp_0", "sp_1")
SP_FS_TP = ("sp_0", "sp_1", "fs", "tp")
F32 = jnp.float32
BF16 = jnp.bfloat16

NORM_EPS = 1e-06
KEY_EPS = 1e-06
GROUP_EPS = 0.00064
DECAY_FLOOR = -104.0

NT = (((1,), (1,)), ((), ()))
TN = (((0,), (0,)), ((), ()))


def ring_shift(array, axis, by):
    devices = lax.axis_size(axis)
    return lax.ppermute(array, axis, [(i, (i + by) % devices) for i in range(devices)])


def passed_along(array, axis, by):
    devices = lax.axis_size(axis)
    pairs = [(i, i + by) for i in range(devices) if 0 <= i + by < devices]
    return lax.ppermute(array, axis, pairs)


def from_everyone(array, axis):
    copies = jnp.broadcast_to(array, (lax.axis_size(axis), *array.shape))
    return lax.all_to_all(copies, axis, split_axis=0, concat_axis=0, tiled=True)


class Fetched:
    def __init__(self, source, target, sem):
        self.copy = pltpu.make_async_copy(source, target, sem)
        self.copy.start()
        self.target = target

    def get(self):
        self.copy.wait()
        return self.target


class Stored:
    def __init__(self, ref, target, sem):
        self.ref = ref
        self.copy = pltpu.make_async_copy(ref, target, sem)

    def put(self):
        self.copy.start()


def call(kernel, outs, scratch=(), flops=0, smem=0, far=None, far_out=()):
    far = far or {}

    def run(*args):
        n_in, n_out = len(args), len(outs)
        held = []
        for i in sorted(far):
            rows, width = args[i].shape[-2:]
            if far[i] is not None:
                _, rows, _, width = far[i]
            held.append(pltpu.VMEM((*args[i].shape[:-2], rows, width), args[i].dtype))
        held += [pltpu.VMEM(*outs[i]) for i in far_out]
        ins = [
            pl.BlockSpec(memory_space=pltpu.SMEM)
            if i < smem
            else pl.BlockSpec(memory_space=pltpu.HBM if i in far else pltpu.VMEM)
            for i in range(n_in)
        ]

        def body(*refs):
            refs = list(refs)
            extra = refs[n_in + n_out :]
            sems = extra[len(held)]
            for k, i in enumerate(sorted(far)):
                source = refs[i]
                if far[i] is not None:
                    source = source.at[pl.ds(*far[i][:2]), pl.ds(*far[i][2:])]
                refs[i] = Fetched(source, extra[k], sems.at[k])
            stored = []
            for k, i in enumerate(far_out):
                at = len(far) + k
                stored.append(Stored(extra[at], refs[n_in + i], sems.at[at]))
                refs[n_in + i] = stored[-1]
            kernel(*refs[: n_in + n_out], *extra[len(held) + 1 :])
            for one in stored:
                one.copy.wait()

        args = [
            pltpu.with_memory_space_constraint(a, pltpu.HBM) if i in far else a
            for i, a in enumerate(args)
        ]
        return pl.pallas_call(
            body,
            out_shape=[
                pltpu.HBM(*o) if i in far_out else jax.ShapeDtypeStruct(*o)
                for i, o in enumerate(outs)
            ],
            in_specs=ins,
            out_specs=[
                pl.BlockSpec(memory_space=pltpu.HBM if i in far_out else pltpu.VMEM)
                for i in range(n_out)
            ],
            scratch_shapes=[*held, pltpu.SemaphoreType.DMA((max(1, len(held)),)), *scratch],
            cost_estimate=pl.CostEstimate(flops=flops, bytes_accessed=1 << 21, transcendentals=0),
            compiler_params=pltpu.CompilerParams(vmem_limit_bytes=24 << 20),
        )(*args)

    return run


def dot(a, b, dims=(((1,), (0,)), ((), ()))):
    return lax.dot_general(a.astype(BF16), b.astype(BF16), dims, preferred_element_type=F32)


def running_sums(x, size):
    rows = x.shape[1]
    lane = lax.broadcasted_iota(jnp.int32, x.shape, 1) % size
    total, after = x, x
    step = 1
    while step < size:
        total = total + jnp.where(lane >= step, pltpu.roll(total, step, 1), 0.0)
        after = after + jnp.where(lane < size - step, pltpu.roll(after, rows - step, 1), 0.0)
        step *= 2
    return total, after


def hidden_parts(place, blocks, other, gain):
    x, core = place[0], place[1]
    rows, width = blocks[0].shape
    sums = jnp.zeros((rows, 1), F32)
    for k in range(4):
        mine = blocks[k][...].astype(F32)
        theirs = other[k].astype(F32)
        sums += jnp.sum(mine * mine + theirs * theirs, axis=1, keepdims=True)
    scale = lax.rsqrt(sums / (8 * width) + NORM_EPS)
    for k in range(4):
        chip = lax.rem(x + k, 4)
        for c, block in ((core, blocks[k][...]), (1 - core, other[k])):
            at = pl.multiple_of((chip * 2 + c) * width, width)
            yield at, (block.astype(F32) * scale * gain[:, pl.ds(at, width)]).astype(BF16)


def halo_kernel(place, own, next_, before, across, other, gain, hid):
    width = own.shape[1]
    for at, h in hidden_parts(place, [own, before, across, next_], other, gain):
        hid.ref[:, pl.ds(at, width)] = h
    hid.put()


def hidden_kernel(place, own, next_, before, across, other, gain, down, up, base, hid, decays):
    rows, width = own.shape
    low = jnp.zeros((rows, down.shape[0]), F32)
    for at, h in hidden_parts(place, [own, before, across, next_], other, gain):
        hid.ref[:, pl.ds(at, width)] = h
        low += lax.dot_general(h, down[:, pl.ds(at, width)], NT, preferred_element_type=F32)
    hid.put()
    low = jnp.tanh(low).astype(BF16)
    rate = lax.dot_general(up[...], low, (((0,), (1,)), ((), ())), preferred_element_type=F32)
    heads = base.shape[0]
    base_rows = jnp.concatenate(
        [jnp.broadcast_to(base[h : h + 1, :], (HEAD, base.shape[1])) for h in range(heads)], axis=0
    )
    log_decay = jnp.maximum(-jnp.exp(rate + base_rows), DECAY_FLOOR)
    for k, size in enumerate((CHUNK, HALF)):
        total, after = running_sums(log_decay, size)
        decays.ref[3 * k] = total
        decays.ref[3 * k + 1] = total - log_decay
        decays.ref[3 * k + 2] = after - log_decay
    decays.put()


def as_column(row):
    return jnp.broadcast_to(row, (8, row.shape[1])).T[:, :1]


def head_rows(h):
    return slice(h * HEAD, (h + 1) * HEAD)


def pair_tables(left, right, start, end, near_start, near_end, rate, first, heads):
    rows = left.shape[1]
    at_j = lax.broadcasted_iota(jnp.int32, (CHUNK, rows), 0)
    at_i = lax.broadcasted_iota(jnp.int32, (CHUNK, rows), 1) % CHUNK
    dist = jnp.where(at_i // HALF == at_j // HALF, at_i - at_j, -1)
    all_j = lax.broadcasted_iota(jnp.int32, (rows, rows), 0)
    all_i = lax.broadcasted_iota(jnp.int32, (rows, rows), 1)
    same = all_i // CHUNK == all_j // CHUNK
    across = same & (all_i // HALF > all_j // HALF)
    plain, rated = [], []
    for h in range(heads):
        sl = head_rows(h)
        l, r, s, e = left[sl, :], right[sl, :], start[sl, :], end[sl, :]
        speed = jnp.broadcast_to(rate[sl, :], l.shape)
        t_plain = jnp.zeros((CHUNK, rows), F32)
        t_rated = jnp.zeros((CHUNK, rows), F32)
        for d in range(first, HALF):
            rd = r if d == 0 else pltpu.roll(r, d, 1)
            ed = e if d == 0 else pltpu.roll(e, d, 1)
            x = l * rd * jnp.exp(s - ed)
            here = dist == d
            t_plain = jnp.where(here, jnp.sum(x, axis=0, keepdims=True), t_plain)
            t_rated = jnp.where(here, jnp.sum(x * speed, axis=0, keepdims=True), t_rated)
        later = l * jnp.exp(near_start[sl, :])
        earlier = r * jnp.exp(near_end[sl, :])
        for table, weight, out in ((t_plain, earlier, plain), (t_rated, earlier * speed, rated)):
            far = dot(weight, later, TN)
            tall = jnp.concatenate([table] * (rows // CHUNK), axis=0)
            out.append(jnp.where(across, far, jnp.where(same, tall, 0.0)).astype(BF16))
    return plain, rated


def by_chunk(array):
    rows = array.shape[1]
    chunk = lax.broadcasted_iota(jnp.int32, array.shape, 1) // CHUNK
    return jnp.concatenate(
        [jnp.where(chunk == c, array, 0.0).astype(BF16) for c in range(rows // CHUNK)], axis=0
    )


def spread(row):
    eye = (
        lax.broadcasted_iota(jnp.int32, (HEAD, HEAD), 0)
        == lax.broadcasted_iota(jnp.int32, (HEAD, HEAD), 1)
    )
    return jnp.where(eye, row, 0.0)


def followed(state, kept, change, added):
    low = state.astype(BF16)
    new = state * kept + jnp.dot(low, change.astype(BF16), preferred_element_type=F32)
    return new + jnp.concatenate([jnp.zeros((HEAD, HEAD), F32), added], axis=0)


def kept_by(decays, c, h):
    last = c * CHUNK + CHUNK - 1
    return decays[last : last + 1, head_rows(h)]


def state_kernel(hid, w, lr, decays, ends, units, tables, changes, adds, dec):
    rows = dec.shape[0]
    lr = as_column(lr.get()[...])
    span = lr.shape[0]
    heads = span // HEAD
    hid, decays = hid.get(), decays.get()
    kv = jnp.dot(hid[...], w[...], preferred_element_type=F32).astype(BF16).astype(F32)
    kv_t = kv.T
    for h in range(heads):
        k = kv_t[head_rows(h), :]
        square = jnp.sum(k * k, axis=0, keepdims=True) + KEY_EPS
        inv = lax.rsqrt(square)
        units.ref[0, head_rows(h), :] = k * inv
        units.ref[1, head_rows(h), :] = kv_t[span + h * HEAD : span + (h + 1) * HEAD, :] * (square * inv)
    cum, prev = decays[0], decays[1]
    dec[...] = jnp.exp(cum).T
    u = units.ref[0]
    v = units.ref[1]
    plain, rated = pair_tables(u, u, prev, cum, decays[4], decays[5], lr, 1, heads)
    reach = jnp.exp(prev)
    x, q = [], []
    for h in range(heads):
        sl = head_rows(h)
        x.append(jnp.concatenate([-u[sl, :] * reach[sl, :], -dot(v[sl, :], plain[h])], axis=0))
        q.append(-rated[h])
    units.put()
    power = 1
    while power < CHUNK:
        for h in range(heads):
            x[h] = x[h] + dot(x[h], q[h])
        power *= 2
        if power < CHUNK:
            for h in range(heads):
                q[h] = dot(q[h], q[h]).astype(BF16)
    left = jnp.exp(decays[2])
    chunks = rows // CHUNK
    for h in range(heads):
        sl = head_rows(h)
        tables.ref[h] = x[h].astype(BF16)
        out_u = u[sl, :] * left[sl, :]
        out_b = out_u * lr[sl, :]
        g = dot(x[h], by_chunk(out_b), NT)
        changes.ref[h] = g[:HEAD, :].astype(BF16)
        adds.ref[h] = g[HEAD:, :] + dot(v[sl, :], by_chunk(out_u), NT)
    parts = []
    for h in range(heads):
        for c in range(chunks):
            at = slice(c * HEAD, (c + 1) * HEAD)
            parts.append((h, kept_by(dec, c, h), changes.ref[h, :, at].astype(F32), adds.ref[h, :, at]))
    tables.put()
    changes.put()
    adds.put()
    while len(parts) > heads:
        joined = []
        for (h, kept, change, added), (_, kept2, change2, added2) in zip(parts[::2], parts[1::2]):
            both = jnp.concatenate([change + spread(kept), added], axis=0)
            both = followed(both, kept2, change2, added2)
            kept = kept * kept2
            joined.append((h, kept, both[:HEAD, :] - spread(kept), both[HEAD:, :]))
        parts = joined
    packed = jnp.concatenate(
        [jnp.concatenate([change + spread(kept), added], axis=0) for _, kept, change, added in parts],
        axis=1,
    ).astype(BF16)
    for k in range(ends.shape[0]):
        ends[k] = packed


def read_part(reads, lr, decays, units, tables, changes, adds, out):
    rows = reads.shape[0]
    heads = lr.shape[0] // HEAD
    r = reads.T
    cum = decays[0]
    reach = jnp.exp(cum)
    dec = reach.T
    eye = jnp.concatenate([spread(jnp.ones((1, HEAD), F32)), jnp.zeros((HEAD, HEAD), F32)], axis=0)
    starts = [[eye] for _ in range(heads)]
    for c in range(rows // CHUNK - 1):
        at = slice(c * HEAD, (c + 1) * HEAD)
        for h in range(heads):
            starts[h].append(
                followed(starts[h][-1], kept_by(dec, c, h), changes[h, :, at], adds[h, :, at])
            )
    near = decays[3]
    plain, rated = pair_tables(r, units[0], cum, cum, near, decays[5], lr, 0, heads)
    reach = r * reach
    for h in range(heads):
        sl = head_rows(h)
        mixed = dot(tables[h], rated[h])
        query = mixed[:HEAD, :] + reach[sl, :]
        local = mixed[HEAD:, :] + dot(units[1, sl, :], plain[h])
        start = jnp.concatenate([x.astype(BF16) for x in starts[h]], axis=1)
        both = dot(start, by_chunk(query))
        out.ref[h, :HEAD, :] = both[:HEAD, :]
        out.ref[h, HEAD:, :] = both[HEAD:, :] + local
    out.put()


def chain(parts):
    while len(parts) > 1:
        parts = [
            jnp.dot(a.astype(BF16), b[:HEAD, :].astype(BF16), preferred_element_type=F32)
            + jnp.concatenate([jnp.zeros((HEAD, HEAD), F32), b[HEAD:, :]], axis=0)
            for a, b in zip(parts[::2], parts[1::2])
        ]
    return parts[0]


def piece(pieces, k, h):
    return pieces[k, :, head_rows(h)].astype(F32)


def chain_before(place, pieces, h):
    eye = jnp.concatenate([spread(jnp.ones((1, HEAD), F32)), jnp.zeros((HEAD, HEAD), F32)], axis=0)
    devices = pieces.shape[0]
    return chain([jnp.where(k < place, piece(pieces, k, h), eye) for k in range(devices)])


def row_kernel(pieces, total):
    devices, heads = pieces.shape[0], pieces.shape[2] // HEAD
    parts = [chain([piece(pieces, k, h) for k in range(devices)]) for h in range(heads)]
    packed = jnp.concatenate(parts, axis=1).astype(BF16)
    for k in range(total.shape[0]):
        total[k] = packed


def inside_kernel(place, pieces, inside):
    pieces = pieces.get()
    heads = pieces.shape[2] // HEAD
    parts = [chain_before(place[0], pieces, h) for h in range(heads)]
    inside[...] = jnp.concatenate(parts, axis=1).astype(BF16)


def final_kernel(place, pieces, inside, local, gain, att, w, out):
    heads = pieces.shape[2] // HEAD
    state = [chain_before(place[0], pieces, h)[HEAD:, :] for h in range(heads)]
    rows = []
    gain = as_column(gain.get()[...])
    inside, local = inside.get(), local.get()
    for h in range(heads):
        near = inside[:, head_rows(h)]
        start = jnp.dot(state[h].astype(BF16), near[:HEAD, :], preferred_element_type=F32)
        start = start + near[HEAD:, :].astype(F32)
        y = dot(start, local[h, :HEAD, :]) + local[h, HEAD:, :]
        centered = y - jnp.mean(y, axis=0, keepdims=True)
        variance = jnp.mean(centered * centered, axis=0, keepdims=True)
        rows.append(centered * lax.rsqrt(variance + GROUP_EPS) * gain[head_rows(h), :])
    rec = jnp.concatenate(rows, axis=0).T.astype(BF16)
    mix = jnp.concatenate([att.get()[...], rec], axis=1)
    w = w.get()
    groups, width = out.shape[0], 512
    size = out.shape[1]
    for n in range(w.shape[0] // width):
        at = slice(n * width, (n + 1) * width)
        part = lax.dot_general(mix, w[at, :], NT, preferred_element_type=F32).astype(BF16)
        for g in range(groups):
            out[g % 2 * (groups // 2) + g // 2, :, at] = part[g * size : (g + 1) * size, :]


def head_rms(values, gain):
    heads = []
    for h in range(values.shape[1] // HEAD):
        x = values[:, head_rows(h)]
        mean_sq = jnp.mean(x * x, axis=1, keepdims=True)
        heads.append((x * lax.rsqrt(mean_sq + NORM_EPS) * gain).astype(BF16))
    return heads


def attention_part(at_start, sink, queries, keys, values, out, lse):
    shape = (2 * WINDOW, WINDOW)
    key_at = lax.broadcasted_iota(jnp.int32, shape, 0)
    lag = lax.broadcasted_iota(jnp.int32, shape, 1) + WINDOW - key_at
    near = (lag >= 0) & (lag < WINDOW)
    for n in range(queries[0].shape[0] // WINDOW):
        at = slice(n * WINDOW, (n + 1) * WINDOW)
        band = slice(n * WINDOW, (n + 2) * WINDOW)
        allowed = near & ((key_at >= WINDOW) | jnp.logical_not(at_start)) if n == 0 else near
        tiles = []
        for h, query in enumerate(queries):
            score = lax.dot_general(
                keys[band, :], query[at, :], NT, preferred_element_type=F32
            ) * (1.0 / math.sqrt(HEAD))
            score = jnp.where(allowed, score, -jnp.inf)
            top = jnp.maximum(jnp.max(score, axis=0, keepdims=True), sink[h])
            weight = jnp.exp(score - top)
            total = jnp.sum(weight, axis=0, keepdims=True) + jnp.exp(sink[h] - top)
            lse[h : h + 1, at] = top + jnp.log(total)
            probs = (weight / total).astype(BF16)
            mixed = lax.dot_general(probs, values[band, :], TN, preferred_element_type=F32)
            tiles.append(mixed.astype(BF16))
        out.ref[at, :] = jnp.concatenate(tiles, axis=1)
    out.put()


def late_kernel(place, sink, hid, halo, w, query_gain, key_gain, lr, decays, units, tables, changes, adds, local, mix, lse):
    q_w = mix.ref.shape[1]
    lr = as_column(lr.get()[...])
    hid, w, halo = hid.get(), w.get(), halo.get()
    own = jnp.dot(hid[...], w[...], preferred_element_type=F32).astype(BF16)
    whole = own.shape[1] - lr.shape[0]
    ahead = jnp.dot(halo[...], w[:, q_w:whole], preferred_element_type=F32).astype(BF16)
    made = [ref.get() for ref in (decays, units, tables, changes, adds)]
    read_part(own[:, whole:].astype(F32), lr, *made, local)
    queries = head_rms(own[:, :q_w].astype(F32), query_gain[...])
    both = jnp.concatenate([ahead, own[:, q_w:whole]], axis=0)
    (keys,) = head_rms(both[:, :HEAD].astype(F32), key_gain[...])
    attention_part(place[0] == 0, sink, queries, keys, both[:, HEAD:], mix, lse)


def per_device(
    tokens,
    norm_gain,
    query_w,
    key_w,
    value_w,
    recept_w,
    rec_key_w,
    rec_value_w,
    decay_down,
    decay_up,
    decay_base,
    learn_rate,
    query_gain,
    key_gain,
    sink_logit,
    group_gain,
    out_att_w,
    out_rec_w,
):
    rows = tokens.shape[0]
    span = recept_w.shape[1]
    heads = span // HEAD
    features = norm_gain.shape[0]
    groups = lax.axis_size(("fs", "tp"))
    place_zy = [lax.axis_index(a).astype(jnp.int32).reshape(1) for a in SP]

    own = jnp.concatenate(
        [rec_key_w, rec_value_w, query_w, key_w, value_w, recept_w, out_att_w.T, out_rec_w.T], axis=1
    )
    column = from_everyone(own, "sp_1").reshape(-1, own.shape[1])
    state_w = from_everyone(column[:, : 2 * span], "sp_0").reshape(features, 2 * span)
    before = ring_shift(tokens, "fs", -1)
    across = ring_shift(tokens, "fs", 2)
    next_ = ring_shift(tokens, "fs", 1)
    ahead = passed_along(tokens[rows - WINDOW :], SP, 1)
    other = ring_shift(jnp.stack([tokens, before, across, next_]), "tp", 1)


    place_xc = jnp.stack([lax.axis_index("fs"), lax.axis_index("tp")]).astype(jnp.int32)
    decay_cols = lax.dynamic_slice_in_dim(
        decay_up, lax.axis_index(("fs", "tp")) * span, span, 1
    )
    flat = (span, rows)
    hid, decays = call(
        hidden_kernel, [((rows, features), BF16), ((6, *flat), F32)], smem=1, flops=1 << 27, far_out=(0, 1)
    )(
        place_xc, tokens, next_, before, across, other, norm_gain.reshape(1, -1), decay_down.T, decay_cols, decay_base
    )


    held, hid = lax.optimization_barrier((column[:, 2 * span :], hid))
    other_w = lax.all_gather(held, "sp_0", axis=0, tiled=True)

    ahead, hid = lax.optimization_barrier((ahead, hid))
    halo_before = ring_shift(ahead, "fs", -1)
    halo_across = ring_shift(ahead, "fs", 2)
    halo_next = ring_shift(ahead, "fs", 1)
    halo_other = ring_shift(jnp.stack([ahead, halo_before, halo_across, halo_next]), "tp", 1)
    (halo,) = call(
        halo_kernel, [((WINDOW, features), BF16)], smem=1, flops=1 << 26, far_out=(0,)
    )(place_xc, ahead, halo_next, halo_before, halo_across, halo_other, norm_gain.reshape(1, -1))

    lr = learn_rate.reshape(1, span)
    chunks = rows // CHUNK
    pair = (2 * HEAD, span)
    ends, *made = call(
        state_kernel,
        [
            ((lax.axis_size("sp_1"), *pair), BF16),
            ((2, *flat), F32),
            ((heads, 2 * HEAD, rows), BF16),
            ((heads, HEAD, chunks * HEAD), BF16),
            ((heads, HEAD, chunks * HEAD), F32),
        ],
        scratch=[pltpu.VMEM((rows, span), F32)],
        flops=1 << 31,
        far={0: None, 2: None, 3: None},
        far_out=(1, 2, 3, 4),
    )(hid, state_w, lr, decays)

    row_pieces = lax.all_to_all(ends, "sp_1", 0, 0, tiled=True)
    (row_total,) = call(row_kernel, [((lax.axis_size("sp_0"), *pair), BF16)], flops=1 << 27)(row_pieces)
    (inside,) = call(inside_kernel, [(pair, BF16)], smem=1, flops=1 << 27, far={1: None})(place_zy[1], row_pieces)
    all_pieces = lax.all_to_all(row_total, "sp_0", 0, 0, tiled=True)

    q_w, kv_w = query_w.shape[1], key_w.shape[1]
    whole = q_w + 2 * kv_w
    early = whole + span
    place_sp = lax.axis_index(SP).astype(jnp.int32).reshape(1)
    local, att_mix, row_lse = call(
        late_kernel,
        [((heads, 2 * HEAD, rows), F32), ((rows, q_w), BF16), ((q_w // HEAD, rows), F32)],
        smem=2,
        flops=1 << 31,
        far={2: None, 3: None, 4: (0, features, 0, early), **{i: None for i in range(7, 13)}},
        far_out=(0, 1),
    )(
        place_sp, sink_logit, hid, halo, other_w, query_gain.reshape(1, HEAD), key_gain.reshape(1, HEAD),
        lr, decays, *made,
    )

    (partial,) = call(
        final_kernel,
        [((groups, rows // groups, features), BF16)],
        smem=1,
        flops=1 << 30,
        far={2: None, 3: None, 4: None, 5: None, 6: (0, features, early, q_w + span)},
    )(place_zy[0], all_pieces, inside, local, group_gain.reshape(1, span), att_mix, other_w)
    tiles = lax.all_to_all(partial, "tp", 0, 0, tiled=True).reshape(2, groups // 2, -1, features)
    tiles = jnp.sum(tiles.astype(F32), axis=0).astype(BF16)
    tiles = lax.all_to_all(tiles, "fs", 0, 0, tiled=True)
    mixed = jnp.sum(tiles.astype(F32), axis=0).astype(BF16)
    return (mixed, row_lse)


def solution(mesh):
    split = Mesh(
        mesh.devices.reshape(8, 8, mesh.shape["fs"], mesh.shape["tp"]), ("sp_0", "sp_1", "fs", "tp")
    )
    in_specs = (
        P(SP, ("fs", "tp")),
        P(),
        P(SP, ("fs", "tp")),
        P(SP, ("fs", "tp")),
        P(SP, ("fs", "tp")),
        P(SP, ("fs", "tp")),
        P(SP, ("fs", "tp")),
        P(SP, ("fs", "tp")),
        P(),
        P(),
        P(("fs", "tp"), SP),
        P(("fs", "tp")),
        P(),
        P(),
        P(("fs", "tp")),
        P(("fs", "tp")),
        P(("fs", "tp"), SP),
        P(("fs", "tp"), SP),
    )
    out_specs = (P(SP_FS_TP, None), P(("fs", "tp"), SP))

    return jax.shard_map(per_device, mesh=split, in_specs=in_specs, out_specs=out_specs, check_vma=False)
```
